128 devices in a mesh: sp: 32 (over z, y, core), tp: 4 (over x).
Axes of the slice: x: 4, y: 4, z: 4, core: 2. Of those that a mesh axis runs over, the one named last changes fastest.
Arguments:
- conv_input: bfloat16 [16384, 1024], P('sp', 'tp'), may hold values from -6 to 6
- gate_inner: bfloat16 [16384, 1024], P('sp', 'tp'), may hold values from -6 to 6
- gate_outer: bfloat16 [16384, 1024], P('sp', 'tp'), may hold values from -6 to 6
- conv_taps: bfloat16 [3, 1024], P(None, 'tp'), may hold values from -3.5 to 3.5
- doc_ids: int32 [16384], P('sp'), may hold values from 0 to 15, never falling along the last dimension, each value on 1 to 2048 neighbouring positions
- residual_in: bfloat16 [16384, 2048], P(('sp', 'tp')), may hold values from -6 to 6
- out_proj: bfloat16 [1024, 2048], replicated, may hold values from -0.1875 to 0.1875
- norm_gain: float32 [2048], replicated, may hold values from 0.1 to 1.9
- expert_ids: int32 [16384, 2], P(('sp', 'tp')), may hold values from 0 to 127, all different within a row; in each aligned block of 128 rows (0 to 127, 128 to 255, ...) at most 4 rows name the same one
- expert_weights: float32 [16384, 2], P(('sp', 'tp')), may hold values from 0.2 to 1
- gate_proj: bfloat16 [128, 2048, 1024], P(('sp', 'tp')), may hold values from -0.125 to 0.125
- up_proj: bfloat16 [128, 2048, 1024], P(('sp', 'tp')), may hold values from -0.125 to 0.125
- down_proj: bfloat16 [128, 1024, 2048], P(('sp', 'tp')), may hold values from -0.1875 to 0.1875
Outputs:
- layer_out: bfloat16 [16384, 2048], P(('sp', 'tp'))
The draws below stay inside these ranges and needn't reach their ends.
Inputs may be any that keep to these rules, and one draw needn't show every extreme that they name: `doc_ids`: never falls along positions; each document has at most 2048 positions. `expert_ids`: each row names 2 different experts; within the rows of one device, aligned blocks of 128 rows, no expert is named more than 4 times, a bound that some block reaches.
All inputs are finite; a program needn't handle non-finite values.
Results may differ from the reference program's by a relative error of at most 0.009.
Values may be sent and summed in bfloat16 or wider, within the bound.
No kernel may reach another device: no remote copies, remote signals or barrier semaphores. Data moves between devices by JAX's collectives and lax.ppermute only.
A program may use at most 64 MiB of HBM per device.

```python
import math
import jax
import jax.numpy as jnp
import numpy as np
from jax import lax

D = 2048
CONV = 1024
FF = 1024
KTAPS = 3
TOPK = 2
TOKENS = 16384
ROWS = 128
EXPERTS = 128
CAP = 4
NDOCS = 16
DOC_MOST = 2048


def steps_of(key, shape, cuts, low, top_value):
    level = 1.0
    for axis_at, shards_of in cuts:
        heights = jax.random.uniform(jax.random.fold_in(jax.random.fold_in(key, 6), axis_at), (shards_of,), jnp.float32, low / len(cuts), top_value / len(cuts))
        level = level * jnp.repeat(jnp.exp(heights), shape[axis_at] // shards_of).reshape((-1,) + (1,) * (len(shape) - 1 - axis_at))
    return level


def length_profile(amount, total, most, skew):
    loads = [(1 << 20) // math.isqrt(standing ** skew) + 1 for standing in range(2, amount + 1)]
    surplus, given = total - most - (amount - 1), [1] * (amount - 1)
    while surplus > 0:
        free = [i for i in range(amount - 1) if given[i] < most]
        pool, left = sum([loads[i] for i in free]), surplus
        for i in free:
            more = min(most - given[i], max(1, left * loads[i] // pool), surplus)
            given[i] = given[i] + more
            surplus = surplus - more
    return np.array([most] + given)


def uneven(stream_key, number_of, total, most, slope):
    if number_of == 2:
        one = jax.random.randint(stream_key, (), max(1, total - most), min(most, total - 1) + 1)
        return jnp.stack([one, total - one])
    lengths = jnp.asarray(length_profile(number_of, total, most, slope), jnp.int32)
    twos = (number_of - 1) // 2
    giver, taker = lengths[1:1 + 2 * twos:2], lengths[2:2 + 2 * twos:2]
    slack = jnp.minimum(giver - 1, most - taker)
    shifted = jax.random.randint(jax.random.fold_in(stream_key, 1), (twos,), 0, 1 << 20) % (slack + 1)
    lengths = lengths.at[1:1 + 2 * twos:2].set(giver - shifted).at[2:2 + 2 * twos:2].set(taker + shifted)
    return lengths[jax.random.permutation(jax.random.fold_in(stream_key, 2), number_of)]


def routed_block(rng, own, number, rows, number_of, top, reach, slope):
    ranking = jax.random.permutation(rng, number_of)
    heavy_load, common = portions_of(number_of, rows * top, reach, slope, True), portions_of(number_of, rows * top, reach, slope, False)
    places = jnp.arange(number_of)

    def named(lengths, offset_by):
        used = int((lengths > 0).sum())
        fixed = max(1, used // 4)
        shifted = fixed + (places - fixed + offset_by * (used - fixed)) % max(1, number_of - fixed)
        return jnp.zeros((number_of,), jnp.int32).at[ranking[jnp.where(places < fixed, places, shifted)]].set(jnp.asarray(lengths, jnp.int32))

    lengths = jnp.where(number % 4 == 0, named(heavy_load, number // 4), named(common, number - number // 4 - 1))
    mixed = jax.random.permutation(jax.random.fold_in(own, 3), number_of)
    source_of, taker = mixed[0:number_of // 2 * 2:2], mixed[1:number_of // 2 * 2:2]
    slack = jnp.minimum(lengths[source_of] - 1, reach - lengths[taker]) // 2
    slack = jnp.where((source_of == ranking[0]) | (taker == ranking[0]) | (lengths[taker] == 0), 0, jnp.maximum(slack, 0))
    shifted = jax.random.randint(jax.random.fold_in(own, 4), (number_of // 2,), 0, 1 << 20) % (slack + 1)
    lengths = lengths.at[source_of].add(-shifted).at[taker].add(shifted)
    members = jnp.searchsorted(jnp.cumsum(lengths), jnp.arange(rows * top), side="right").astype(jnp.int32)
    table = members.reshape(top, rows).T
    table = table[jax.random.permutation(jax.random.fold_in(own, 1), rows)]
    offset_by = jax.random.randint(jax.random.fold_in(own, 2), (rows, 1), 0, top)
    return jnp.take_along_axis(table, (jnp.arange(top)[None, :] + offset_by) % top, axis=1)


def portions_of(amount, total, limit, skew, full):
    portions = [(1 << 20) // math.isqrt(rank ** skew) + 1 for rank in range(1, amount + 1)]
    largest = limit if full else min(limit, max(-(-total // amount), total * portions[0] // sum(portions)))
    least = 1 if total - largest >= amount - 1 else 0
    counts, rest = [largest] + [least] * (amount - 1), total - largest - least * (amount - 1)
    while rest > 0:
        free = [i for i in range(1, amount) if counts[i] < largest] or [i for i in range(1, amount) if counts[i] < limit]
        whole, budget = sum([portions[i] for i in free]), rest
        for i in free:
            extra = min(limit - counts[i], max(1, budget * portions[i] // whole), rest)
            counts[i] = counts[i] + extra
            rest = rest - extra
    return np.array(counts)


def gaussian(rng, dims, scale, reach, pieces=(), kind=jnp.bfloat16):
    result = jax.random.normal(rng, dims, jnp.float32) * scale
    if len(pieces) > 0:
        result = steps_of(rng, dims, pieces, -0.22, 0.18) * result
    return jnp.clip(result, min=-reach, max=reach).astype(kind)


def setup_inputs(seed: int = 0) -> dict:
    splits = jax.random.split(jax.random.key(seed), 14)
    conv_input = gaussian(splits[0], (TOKENS, CONV), 1.0, 6.0, ((0, 32), (1, 4)))
    gate_inner = gaussian(splits[1], (TOKENS, CONV), 1.0, 6.0, ((0, 32), (1, 4)))
    gate_outer = gaussian(splits[2], (TOKENS, CONV), 1.0, 6.0, ((0, 32), (1, 4)))
    conv_taps = gaussian(splits[3], (KTAPS, CONV), KTAPS ** -0.5, 3.5, ((1, 4),))
    doc_ids = jnp.searchsorted(jnp.cumsum(uneven(splits[4], NDOCS, TOKENS, DOC_MOST, 0)), jnp.arange(TOKENS), side="right").astype(jnp.int32)
    residual_in = gaussian(splits[5], (TOKENS, D), 1.0, 6.0, ((0, 128),))
    out_proj = gaussian(splits[6], (CONV, D), CONV ** -0.5, 0.1875)
    norm_gain = jnp.clip(1.0 + 0.18 * jax.random.normal(splits[7], (D,), jnp.float32), 0.1, 1.9)
    expert_ids_keys = jax.random.split(jax.random.fold_in(splits[8], 1), TOKENS // ROWS)
    expert_ids_turns = jax.random.permutation(jax.random.fold_in(splits[8], 3), TOKENS // ROWS)
    expert_ids = jax.vmap(lambda own, number: routed_block(jax.random.fold_in(splits[8], 2), own, number, ROWS, EXPERTS, TOPK, CAP, 1))(expert_ids_keys, expert_ids_turns).reshape((TOKENS, TOPK))
    expert_weights = jnp.clip(0.2 + 0.8 * jax.random.uniform(splits[9], (TOKENS, TOPK), jnp.float32) ** steps_of(splits[9], (TOKENS, TOPK), ((0, 128),), -0.2, 0.2), 0.2, 1.0)
    gate_proj = gaussian(splits[10], (EXPERTS, D, FF), D ** -0.5, 0.125, ((0, 128),))
    up_proj = gaussian(splits[11], (EXPERTS, D, FF), D ** -0.5, 0.125, ((0, 128),))
    down_proj = gaussian(splits[12], (EXPERTS, FF, D), FF ** -0.5, 0.1875, ((0, 128),))
    return {"conv_input": conv_input, "gate_inner": gate_inner, "gate_outer": gate_outer, "conv_taps": conv_taps, "doc_ids": doc_ids, "residual_in": residual_in, "out_proj": out_proj, "norm_gain": norm_gain, "expert_ids": expert_ids, "expert_weights": expert_weights, "gate_proj": gate_proj, "up_proj": up_proj, "down_proj": down_proj}


def expert_rows(arrived, gate_weight, up_weight, down_weight):
    gate_value = jnp.dot(arrived, gate_weight, preferred_element_type=jnp.float32)
    up_value = jnp.dot(arrived, up_weight, preferred_element_type=jnp.float32)
    hidden = (jax.nn.silu(gate_value) * up_value).astype(jnp.bfloat16)
    return jnp.dot(hidden, down_weight, preferred_element_type=jnp.float32).astype(jnp.bfloat16)

def reference(conv_input, gate_inner, gate_outer, conv_taps, doc_ids, residual_in, out_proj, norm_gain, expert_ids, expert_weights, gate_proj, up_proj, down_proj):
    inner_prod = conv_input.astype(jnp.float32) * gate_inner.astype(jnp.float32)
    tap_values = conv_taps.astype(jnp.float32)
    channels = inner_prod.shape[1]
    one_rows = jnp.concatenate([jnp.zeros((1, channels), jnp.float32), inner_prod[:-1]], axis=0)
    two_rows = jnp.concatenate([jnp.zeros((2, channels), jnp.float32), inner_prod[:-2]], axis=0)
    one_docs = jnp.concatenate([jnp.full((1,), -1, jnp.int32), doc_ids[:-1]], axis=0)
    two_docs = jnp.concatenate([jnp.full((2,), -1, jnp.int32), doc_ids[:-2]], axis=0)
    one_back = jnp.where((one_docs == doc_ids)[:, None], one_rows, 0.0)
    two_back = jnp.where((two_docs == doc_ids)[:, None], two_rows, 0.0)
    mixed_rows = tap_values[2] * inner_prod + tap_values[1] * one_back + tap_values[0] * two_back
    conv_out = (gate_outer.astype(jnp.float32) * mixed_rows).astype(jnp.bfloat16)
    mix = jnp.dot(conv_out, out_proj, preferred_element_type=jnp.float32).astype(jnp.bfloat16)
    carried = residual_in.astype(jnp.float32) + mix.astype(jnp.float32)
    normed = (carried * lax.rsqrt(lax.optimization_barrier(jnp.mean(carried * carried, axis=1, keepdims=True)) + 1e-06) * norm_gain).astype(jnp.bfloat16)
    choose = expert_ids.shape[1]
    blocks = TOKENS // ROWS
    block_ids = expert_ids.reshape(blocks, ROWS * choose)
    onehot = (block_ids[:, :, None] == jnp.arange(EXPERTS, dtype=jnp.int32)[None, None, :]).astype(jnp.int32)
    slot_rank = lax.optimization_barrier(jnp.sum((jnp.cumsum(onehot, axis=1) - 1) * onehot, axis=2))
    block_index = jnp.arange(blocks, dtype=jnp.int32)[:, None]
    target = (block_ids * (blocks * CAP) + block_index * CAP + slot_rank).reshape(-1).astype(jnp.int32)
    sources = jnp.repeat(normed, choose, axis=0)
    buffer = jnp.zeros((EXPERTS * blocks * CAP, D), jnp.bfloat16).at[target].set(sources)
    buffer = buffer.reshape(EXPERTS, blocks * CAP, D)

    def serve(operands):
        return expert_rows(operands[0], operands[1], operands[2], operands[3])
    results = lax.map(serve, (buffer, gate_proj, up_proj, down_proj))
    picked = results.reshape(-1, D)[target].reshape(TOKENS, choose, D).astype(jnp.float32)
    combined = carried + lax.optimization_barrier(jnp.sum(expert_weights[:, :, None] * picked, axis=1))
    return combined.astype(jnp.bfloat16)
```

```python
import functools
import jax
import jax.numpy as jnp
from jax import lax
from jax.experimental import pallas as pl
from jax.experimental.pallas import tpu as pltpu
from jax.sharding import PartitionSpec as P

F32 = jnp.float32
BF16 = jnp.bfloat16
VM = pl.BlockSpec(memory_space=pltpu.VMEM)
SM = pl.BlockSpec(memory_space=pltpu.SMEM)
ANY = pl.BlockSpec(memory_space=pl.ANY)


def dot(a, b):
    return jnp.dot(a, b, preferred_element_type=F32)


def conv_kernel(place, earlier, x, g_in, g_out, taps, docs, o0, o1, o2, o3, prod, doc_col):
    rows = x.shape[0]
    part = o0.shape[0]
    prod[0:8, :] = jnp.concatenate([jnp.zeros((6, x.shape[1]), F32), earlier[0:2, :]], axis=0)
    prod[8:, :] = x[...].astype(F32) * g_in[...].astype(F32)
    doc_col[0:8, :] = jnp.concatenate(
        [jnp.zeros((6, 128), F32), earlier[2:4, 0:128]], axis=0
    )
    for block in range(rows // 128):
        line = jnp.broadcast_to(docs[block : block + 1, :].astype(F32), (128, 128))
        doc_col[8 + 128 * block : 136 + 128 * block, :] = line.T
    t0 = taps[0:1, :].astype(F32)
    t1 = taps[1:2, :].astype(F32)
    t2 = taps[2:3, :].astype(F32)
    here = place[0]
    for shift, out in enumerate((o0, o1, o2, o3)):
        start = pl.multiple_of(lax.rem(here + shift, 4) * part, part)
        window = prod[pl.ds(start, part + 8), :]
        ids = doc_col[pl.ds(start, part + 8), :]
        cur = ids[8:]
        same1 = ids[7:-1] == cur
        same2 = ids[6:-2] == cur
        for half in range(x.shape[1] // 128):
            c = slice(128 * half, 128 * half + 128)
            back1 = jnp.where(same1, window[7:-1, c], 0.0)
            back2 = jnp.where(same2, window[6:-2, c], 0.0)
            mixed = t2[:, c] * window[8:, c] + t1[:, c] * back1 + t0[:, c] * back2
            out[:, c] = (g_out[pl.ds(start, part), c].astype(F32) * mixed).astype(BF16)


def slots_kernel(ids, tgt):
    tokens = ids.shape[1]
    first = ids[0:1, :]
    second = ids[1:2, :]
    expert = lax.broadcasted_iota(jnp.int32, (128, tokens), 0)
    m0 = (expert == first).astype(F32)
    m1 = (expert == second).astype(F32)
    r = lax.broadcasted_iota(jnp.int32, (tokens, tokens), 0)
    c = lax.broadcasted_iota(jnp.int32, (tokens, tokens), 1)
    before = (r < c).astype(BF16)
    n0 = dot(m0.astype(BF16), before)
    n1 = dot(m1.astype(BF16), before) + jnp.sum(m0, axis=1, keepdims=True)
    rank0 = jnp.sum(m0 * n0, axis=0, keepdims=True).astype(jnp.int32)
    rank1 = jnp.sum(m1 * n1, axis=0, keepdims=True).astype(jnp.int32)
    tgt[0:1, :] = first * 8 + rank0
    tgt[1:2, :] = second * 8 + rank1


def mix_kernel(place, r0, r1, r2, r3, residual, proj, gain, tgt, buf, carried, halves, onehot):
    here = place[0]
    width = residual.shape[1]
    half = width // 2
    tokens = residual.shape[0]
    row = lax.broadcasted_iota(jnp.int32, (buf.shape[0], tokens), 0)
    a, b = tgt[0:1, :], tgt[1:2, :]
    onehot[:, 0:tokens] = ((row == a) | (row == b)).astype(F32).astype(BF16)
    onehot[:, tokens:] = ((row == a + 4) | (row == b + 4)).astype(F32).astype(BF16)
    step = 512
    total = jnp.zeros((tokens, 1), F32)
    for n in range(width // step):
        c = slice(n * step, n * step + step)
        acc = None
        for shift, part in enumerate((r0, r1, r2, r3)):
            depth = part.shape[1]
            start = pl.multiple_of(lax.rem(here + 4 - shift, 4) * depth, depth)
            term = dot(part[...], proj[pl.ds(start, depth), c])
            acc = term if acc is None else acc + term
        value = residual[:, c].astype(F32) + acc.astype(BF16).astype(F32)
        carried[:, c] = value
        total = total + jnp.sum(value * value, axis=1, keepdims=True)
    scale = lax.rsqrt(total * (1.0 / width) + 1e-06)
    for n in range(width // step):
        c = slice(n * step, n * step + step)
        value = (carried[:, c] * scale * gain[:, c]).astype(BF16)
        h = (n * step) // half
        halves[h * tokens : (h + 1) * tokens, n * step - h * half : n * step - h * half + step] = value
    for n in range(half // 256):
        c = slice(n * 256, n * 256 + 256)
        buf[:, c] = dot(onehot[...], halves[:, c]).astype(BF16)


def expert_kernel(arrived, wg, wu, wd, out, av, gv, uv, dv, xv, hv, ov, sem_a, sem_g, sem_u, sem_d, sem_o):
    rows, half = av.shape
    depth, hidden = gv.shape
    blocks = hidden // 256
    cols = [slice(256 * j, 256 * j + 256) for j in range(blocks)]
    copies_a = [pltpu.make_async_copy(arrived.at[:, c], av.at[:, c], sem_a.at[j]) for j, c in enumerate(cols)]
    copies_g = [pltpu.make_async_copy(wg.at[:, c], gv.at[:, c], sem_g.at[j]) for j, c in enumerate(cols)]
    copies_u = [pltpu.make_async_copy(wu.at[:, c], uv.at[:, c], sem_u.at[j]) for j, c in enumerate(cols)]
    cols_d = [slice(512 * j, 512 * j + 512) for j in range(blocks)]
    copies_d = [pltpu.make_async_copy(wd.at[:, c], dv.at[:, c], sem_d.at[j]) for j, c in enumerate((cols_d[0], cols_d[2], cols_d[1], cols_d[3]))]
    for copy in copies_a:
        copy.start()
    for a, b in zip(copies_g, copies_u):
        a.start()
        b.start()
    for copy in copies_d:
        copy.start()
    low = lax.broadcasted_iota(jnp.int32, (rows // 16, 8, 256), 1) < 4
    for j, c in enumerate(cols):
        copies_a[j].wait()
        value = av[:, c].astype(F32).reshape(rows // 16, 2, 8, 256)
        even, odd = value[:, 0], value[:, 1]
        lo = jnp.where(low, even, pltpu.roll(odd, 4, 1))
        hi = jnp.where(low, pltpu.roll(even, 4, 1), odd)
        xv[:, c] = lo.reshape(rows // 2, 256).astype(BF16)
        xv[:, half + 256 * j : half + 256 * j + 256] = hi.reshape(rows // 2, 256).astype(BF16)
    for j, c in enumerate(cols):
        copies_g[j].wait()
        copies_u[j].wait()
        gate = dot(xv[...], gv[:, c])
        up = dot(xv[...], uv[:, c])
        hv[:, c] = (gate / (1.0 + jnp.exp(-gate)) * up).astype(BF16)
    outs = []
    for j, c in enumerate(cols):
        if j % 2 == 0:
            copies_d[j].wait()
            copies_d[j + 1].wait()
        lo = dot(hv[...], dv[:, c]).reshape(rows // 16, 8, 256)
        hi = dot(hv[...], dv[:, half + 256 * j : half + 256 * j + 256]).reshape(rows // 16, 8, 256)
        even = jnp.where(low, lo, pltpu.roll(hi, 4, 1))
        odd = jnp.where(low, pltpu.roll(lo, 4, 1), hi)
        ov[:, c] = jnp.stack([even, odd], axis=1).reshape(rows, 256).astype(BF16)
        copy = pltpu.make_async_copy(ov.at[:, c], out.at[:, c], sem_o.at[j])
        copy.start()
        outs.append(copy)
    for copy in outs:
        copy.wait()


def combine_kernel(returned, carried, tgt, weights, out, pick):
    tokens = carried.shape[0]
    rows, half = returned.shape
    for k in range(2):
        line = jnp.broadcast_to(tgt[k : k + 1, :].astype(F32), (128, tokens)).T
        for n in range(rows // 128):
            lane = (lax.broadcasted_iota(jnp.int32, (tokens, 128), 1) + 128 * n).astype(F32)
            c = slice(128 * n, 128 * n + 128)
            pick[0, k * tokens : (k + 1) * tokens, c] = (line == lane).astype(F32).astype(BF16)
            pick[1, k * tokens : (k + 1) * tokens, c] = (line + 4.0 == lane).astype(F32).astype(BF16)
    w = [jnp.broadcast_to(weights[k : k + 1, :], (128, tokens)).T[:, 0:1] for k in range(2)]
    for h in range(2):
        for n in range(half // 256):
            c = slice(256 * n, 256 * n + 256)
            d = slice(h * half + 256 * n, h * half + 256 * n + 256)
            both = dot(pick[h], returned[:, c])
            out[:, d] = (carried[:, d] + (w[0] * both[:tokens] + w[1] * both[tokens:])).astype(BF16)


def call(kernel, out_shape, in_specs, out_specs, scratch, vmem_mib, flops=0, nbytes=0, name=None):
    return pl.pallas_call(
        kernel,
        out_shape=out_shape,
        in_specs=in_specs,
        out_specs=out_specs,
        scratch_shapes=scratch,
        name=name,
        compiler_params=pltpu.CompilerParams(vmem_limit_bytes=vmem_mib << 20),
        cost_estimate=pl.CostEstimate(flops=flops, bytes_accessed=nbytes, transcendentals=0),
    )


def shape(dims, kind):
    return jax.ShapeDtypeStruct(dims, kind)


def on_device(conv_input, gate_inner, gate_outer, conv_taps, doc_ids, residual_in, out_proj,
              norm_gain, expert_ids, expert_weights, gate_proj, up_proj, down_proj):
    length, channels = conv_input.shape
    tokens, width = residual_in.shape
    sp_count = lax.axis_size("sp")
    tp_count = lax.axis_size("tp")
    experts = sp_count * tp_count
    place = lax.axis_index("tp").reshape(1)
    tail = conv_input[-2:].astype(F32) * gate_inner[-2:].astype(F32)
    tail_docs = jnp.broadcast_to(doc_ids[-2:].astype(F32)[:, None], (2, channels))
    earlier = lax.ppermute(
        jnp.concatenate([tail, tail_docs], axis=0), "sp", [(i, i + 1) for i in range(sp_count - 1)]
    )
    tgt = call(
        slots_kernel, shape((2, tokens), jnp.int32), [VM], VM, [], 8, 1 << 22, 1 << 16, name="slots"
    )(expert_ids.T)
    piece = shape((tokens, channels), BF16)
    sent = call(
        conv_kernel, (piece,) * 4, [SM] + [VM] * 6, (VM,) * 4,
        [pltpu.VMEM((length + 8, channels), F32), pltpu.VMEM((length + 8, 128), F32)],
        16, 1 << 22, 1 << 20, name="conv",
    )(place, earlier, conv_input, gate_inner, gate_outer, conv_taps, doc_ids.reshape(-1, 128))
    parts = [sent[0]] + [
        lax.ppermute(sent[d], "tp", [(i, (i + d) % tp_count) for i in range(tp_count)])
        for d in range(1, tp_count)
    ]
    rows = experts * 8
    half = width // 2
    buf, carried = call(
        mix_kernel, (shape((rows, half), BF16), shape((tokens, width), F32)),
        [SM] + [VM] * 8, (VM, VM),
        [pltpu.VMEM((2 * tokens, half), BF16), pltpu.VMEM((rows, 2 * tokens), BF16)],
        32, 1 << 30, 1 << 23, name="mix",
    )(place, *parts, residual_in, out_proj, norm_gain.reshape(1, -1), tgt)
    arrived = lax.all_to_all(buf.reshape(experts, 8, half), ("sp", "tp"), split_axis=0, concat_axis=0, tiled=True)
    hidden = gate_proj.shape[2]
    dma = pltpu.SemaphoreType.DMA((hidden // 256,))
    result = call(
        expert_kernel, shape((rows, half), BF16), [ANY] * 4, ANY,
        [
            pltpu.VMEM((rows, half), BF16),
            pltpu.VMEM((width, hidden), BF16),
            pltpu.VMEM((width, hidden), BF16),
            pltpu.VMEM((hidden, width), BF16),
            pltpu.VMEM((rows // 2, width), BF16),
            pltpu.VMEM((rows // 2, hidden), BF16),
            pltpu.VMEM((rows, half), BF16),
        ] + [dma] * 5,
        48, 6 << 30, 1 << 24, name="experts",
    )(arrived.reshape(rows, half), gate_proj[0], up_proj[0], down_proj[0])
    returned = lax.all_to_all(result.reshape(experts, 8, half), ("sp", "tp"), split_axis=0, concat_axis=0, tiled=True)
    return call(
        combine_kernel, shape((tokens, width), BF16), [VM] * 4, VM,
        [pltpu.VMEM((2, 2 * tokens, rows), BF16)],
        32, 1 << 30, 1 << 22, name="combine",
    )(returned.reshape(rows, half), carried, tgt, expert_weights.T)


def solution(mesh):
    both = ("sp", "tp")
    in_specs = (
        P("sp", "tp"),
        P("sp", "tp"),
        P("sp", "tp"),
        P(None, "tp"),
        P("sp"),
        P(both, None),
        P(),
        P(),
        P(both, None),
        P(both, None),
        P(both, None, None),
        P(both, None, None),
        P(both, None, None),
    )
    return jax.shard_map(
        on_device, mesh=mesh, in_specs=in_specs, out_specs=P(both, None), check_vma=False
    )
```

```python
import functools
import jax
import jax.numpy as jnp
from jax import lax
from jax.experimental import pallas as pl
from jax.experimental.pallas import tpu as pltpu
from jax.sharding import PartitionSpec as P

F32 = jnp.float32
BF16 = jnp.bfloat16
VM = pl.BlockSpec(memory_space=pltpu.VMEM)
SM = pl.BlockSpec(memory_space=pltpu.SMEM)
HB = pl.BlockSpec(memory_space=pl.ANY)


def dot(a, b):
    return jnp.dot(a, b, preferred_element_type=F32)


def edge_kernel(x, g_in, docs, out, xv, gv, dv, sem):
    rows = x.shape[0]
    copies = [
        pltpu.make_async_copy(x.at[rows - 16 :, :], xv, sem.at[0]),
        pltpu.make_async_copy(g_in.at[rows - 16 :, :], gv, sem.at[1]),
        pltpu.make_async_copy(docs, dv, sem.at[2]),
    ]
    for copy in copies:
        copy.start()
    for copy in copies:
        copy.wait()
    prod = xv[...].astype(F32) * gv[...].astype(F32)
    last = dv.shape[0] - 1
    ids = jnp.broadcast_to(dv[last : last + 1, :].astype(F32), (128, 128)).T
    out[0:2, :] = prod[14:16, :]
    for c in range(out.shape[1] // 128):
        out[2:4, 128 * c : 128 * c + 128] = ids[126:128, :]


def load_kernel(*refs):
    count = (len(refs) - 1) // 2
    sem = refs[-1]
    copies = [pltpu.make_async_copy(refs[i], refs[count + i], sem.at[i]) for i in range(count)]
    for copy in copies:
        copy.start()
    for copy in copies:
        copy.wait()


def conv_kernel(place, earlier, x, g_in, g_out, taps, docs, o0, o1, o2, o3, prod, doc_col):
    rows = x.shape[0]
    part = o0.shape[0]
    prod[0:8, :] = jnp.concatenate([jnp.zeros((6, x.shape[1]), F32), earlier[0:2, :]], axis=0)
    prod[8:, :] = x[...].astype(F32) * g_in[...].astype(F32)
    doc_col[0:8, :] = jnp.concatenate(
        [jnp.zeros((6, 128), F32), earlier[2:4, 0:128]], axis=0
    )
    for block in range(rows // 128):
        line = jnp.broadcast_to(docs[block : block + 1, :].astype(F32), (128, 128))
        doc_col[8 + 128 * block : 136 + 128 * block, :] = line.T
    t0 = taps[0:1, :].astype(F32)
    t1 = taps[1:2, :].astype(F32)
    t2 = taps[2:3, :].astype(F32)
    here = place[0]
    for shift, out in enumerate((o0, o1, o2, o3)):
        start = pl.multiple_of(lax.rem(here + shift, 4) * part, part)
        window = prod[pl.ds(start, part + 8), :]
        ids = doc_col[pl.ds(start, part + 8), :]
        cur = ids[8:]
        same1 = ids[7:-1] == cur
        same2 = ids[6:-2] == cur
        for half in range(x.shape[1] // 128):
            c = slice(128 * half, 128 * half + 128)
            back1 = jnp.where(same1, window[7:-1, c], 0.0)
            back2 = jnp.where(same2, window[6:-2, c], 0.0)
            mixed = t2[:, c] * window[8:, c] + t1[:, c] * back1 + t0[:, c] * back2
            out[:, c] = (g_out[pl.ds(start, part), c].astype(F32) * mixed).astype(BF16)


def slots_kernel(ids, proj, residual, gain, tgt, proj_v, residual_v, gain_v, iv, sem):
    copies = [
        pltpu.make_async_copy(ids, iv, sem.at[0]),
        pltpu.make_async_copy(proj, proj_v, sem.at[1]),
        pltpu.make_async_copy(residual, residual_v, sem.at[2]),
        pltpu.make_async_copy(gain, gain_v, sem.at[3]),
    ]
    for copy in copies:
        copy.start()
    copies[0].wait()
    tokens = ids.shape[1]
    first = iv[0:1, :]
    second = iv[1:2, :]
    expert = lax.broadcasted_iota(jnp.int32, (128, tokens), 0)
    m0 = (expert == first).astype(F32)
    m1 = (expert == second).astype(F32)
    r = lax.broadcasted_iota(jnp.int32, (tokens, tokens), 0)
    c = lax.broadcasted_iota(jnp.int32, (tokens, tokens), 1)
    before = (r < c).astype(F32).astype(BF16)
    n0 = dot(m0.astype(BF16), before)
    n1 = dot(m1.astype(BF16), before) + jnp.sum(m0, axis=1, keepdims=True)
    rank0 = jnp.sum(m0 * n0, axis=0, keepdims=True).astype(jnp.int32)
    rank1 = jnp.sum(m1 * n1, axis=0, keepdims=True).astype(jnp.int32)
    tgt[0:1, :] = first * 8 + rank0
    tgt[1:2, :] = second * 8 + rank1
    for copy in copies[1:]:
        copy.wait()


def mix_kernel(place, r0, r1, r2, r3, residual, proj, gain, tgt, buf, carried, halves, onehot):
    here = place[0]
    width = residual.shape[1]
    half = width // 2
    tokens = residual.shape[0]
    row = lax.broadcasted_iota(jnp.int32, (buf.shape[0], tokens), 0)
    a, b = tgt[0:1, :], tgt[1:2, :]
    onehot[:, 0:tokens] = ((row == a) | (row == b)).astype(F32).astype(BF16)
    onehot[:, tokens:] = ((row == a + 4) | (row == b + 4)).astype(F32).astype(BF16)
    step = 512
    total = jnp.zeros((tokens, 1), F32)
    for n in range(width // step):
        c = slice(n * step, n * step + step)
        acc = None
        for shift, part in enumerate((r0, r1, r2, r3)):
            depth = part.shape[1]
            start = pl.multiple_of(lax.rem(here + 4 - shift, 4) * depth, depth)
            term = dot(part[...], proj[pl.ds(start, depth), c])
            acc = term if acc is None else acc + term
        value = residual[:, c].astype(F32) + acc.astype(BF16).astype(F32)
        carried[:, c] = value
        total = total + jnp.sum(value * value, axis=1, keepdims=True)
    scale = lax.rsqrt(total * (1.0 / width) + 1e-06)
    for n in range(width // step):
        c = slice(n * step, n * step + step)
        value = (carried[:, c] * scale * gain[:, c]).astype(BF16)
        h = (n * step) // half
        halves[h * tokens : (h + 1) * tokens, n * step - h * half : n * step - h * half + step] = value
    for n in range(half // 256):
        c = slice(n * 256, n * 256 + 256)
        buf[:, c] = dot(onehot[...], halves[:, c]).astype(BF16)


def expert_kernel(arrived, wg, wu, wd, out, dv, xv, hv, sem):
    rows, half = arrived.shape
    blocks = wg.shape[1] // 256
    cols = [slice(256 * j, 256 * j + 256) for j in range(blocks)]
    part = dv.shape[0] // blocks
    copies = [
        pltpu.make_async_copy(wd.at[part * j : part * j + part, :], dv.at[part * j : part * j + part, :], sem.at[j])
        for j in range(blocks)
    ]
    for copy in copies:
        copy.start()
    low = lax.broadcasted_iota(jnp.int32, (rows // 16, 8, 256), 1) < 4
    for j, c in enumerate(cols):
        value = arrived[:, c].astype(F32).reshape(rows // 16, 2, 8, 256)
        even, odd = value[:, 0], value[:, 1]
        lo = jnp.where(low, even, pltpu.roll(odd, 4, 1))
        hi = jnp.where(low, pltpu.roll(even, 4, 1), odd)
        xv[:, c] = lo.reshape(rows // 2, 256).astype(BF16)
        xv[:, half + 256 * j : half + 256 * j + 256] = hi.reshape(rows // 2, 256).astype(BF16)
    for j, c in enumerate(cols):
        gate = dot(xv[...], wg[:, c])
        up = dot(xv[...], wu[:, c])
        hv[:, c] = (gate / (1.0 + jnp.exp(-gate)) * up).astype(BF16)
    for copy in copies:
        copy.wait()
    for j, c in enumerate(cols):
        lo = dot(hv[...], dv[:, c]).reshape(rows // 16, 8, 256)
        hi = dot(hv[...], dv[:, half + 256 * j : half + 256 * j + 256]).reshape(rows // 16, 8, 256)
        even = jnp.where(low, lo, pltpu.roll(hi, 4, 1))
        odd = jnp.where(low, pltpu.roll(lo, 4, 1), hi)
        out[:, c] = jnp.stack([even, odd], axis=1).reshape(rows, 256).astype(BF16)


def combine_kernel(returned, carried, tgt, weights, out, pick):
    tokens = carried.shape[0]
    rows, half = returned.shape
    for k in range(2):
        line = jnp.broadcast_to(tgt[k : k + 1, :].astype(F32), (128, tokens)).T
        for n in range(rows // 128):
            lane = (lax.broadcasted_iota(jnp.int32, (tokens, 128), 1) + 128 * n).astype(F32)
            c = slice(128 * n, 128 * n + 128)
            pick[0, k * tokens : (k + 1) * tokens, c] = (line == lane).astype(F32).astype(BF16)
            pick[1, k * tokens : (k + 1) * tokens, c] = (line + 4.0 == lane).astype(F32).astype(BF16)
    w = [jnp.broadcast_to(weights[k : k + 1, :], (128, tokens)).T[:, 0:1] for k in range(2)]
    for h in range(2):
        for n in range(half // 256):
            c = slice(256 * n, 256 * n + 256)
            d = slice(h * half + 256 * n, h * half + 256 * n + 256)
            both = dot(pick[h], returned[:, c])
            out[:, d] = (carried[:, d] + (w[0] * both[:tokens] + w[1] * both[tokens:])).astype(BF16)


def call(kernel, out_shape, in_specs, out_specs, scratch, vmem_mib, flops=0, nbytes=0, name=None):
    return pl.pallas_call(
        kernel,
        out_shape=out_shape,
        in_specs=in_specs,
        out_specs=out_specs,
        scratch_shapes=scratch,
        name=name,
        compiler_params=pltpu.CompilerParams(vmem_limit_bytes=int(vmem_mib * 1048576)),
        cost_estimate=pl.CostEstimate(flops=flops, bytes_accessed=nbytes, transcendentals=0),
    )


def shape(dims, kind):
    return jax.ShapeDtypeStruct(dims, kind)


def load(arrays, vmem_mib, name):
    size = sum(v.size * v.dtype.itemsize for v in arrays)
    return call(
        load_kernel, tuple(pltpu.VMEM(v.shape, v.dtype) for v in arrays), [HB] * len(arrays),
        (VM,) * len(arrays), [pltpu.SemaphoreType.DMA((len(arrays),))], vmem_mib,
        1 << 30, size, name=name,
    )(*arrays)


def on_device(conv_input, gate_inner, gate_outer, conv_taps, doc_ids, residual_in, out_proj,
              norm_gain, expert_ids, expert_weights, gate_proj, up_proj, down_proj):
    length, channels = conv_input.shape
    tokens, width = residual_in.shape
    sp_count = lax.axis_size("sp")
    tp_count = lax.axis_size("tp")
    experts = sp_count * tp_count
    place = lax.axis_index("tp").reshape(1)
    docs = doc_ids.reshape(-1, 128)
    edge = call(
        edge_kernel, pltpu.VMEM((4, channels), F32), [HB] * 3, VM,
        [pltpu.VMEM((16, channels), BF16), pltpu.VMEM((16, channels), BF16),
         pltpu.VMEM(docs.shape, jnp.int32), pltpu.SemaphoreType.DMA((3,))],
        63, 1 << 20, 1 << 16, name="edge",
    )(conv_input, gate_inner, docs)
    earlier = lax.ppermute(edge, "sp", [(i, i + 1) for i in range(sp_count - 1)])
    early = load((conv_input, gate_inner, gate_outer, conv_taps, docs), 62, "early")
    piece = shape((tokens, channels), BF16)
    sent = call(
        conv_kernel, (piece,) * 4, [SM] + [VM] * 6, (VM,) * 4,
        [pltpu.VMEM((length + 8, channels), F32), pltpu.VMEM((length + 8, 128), F32)],
        16, 1 << 22, 1 << 20, name="conv",
    )(place, earlier, *early)
    parts = [sent[0]] + [
        lax.ppermute(sent[d], "tp", [(i, (i + d) % tp_count) for i in range(tp_count)])
        for d in range(1, tp_count)
    ]
    gain = norm_gain.reshape(1, -1)
    tgt, proj_v, residual_v, gain_v = call(
        slots_kernel,
        (pltpu.VMEM((2, tokens), jnp.int32),) + tuple(pltpu.VMEM(v.shape, v.dtype) for v in (out_proj, residual_in, gain)),
        [HB] * 4, (VM,) * 4,
        [pltpu.VMEM((2, tokens), jnp.int32), pltpu.SemaphoreType.DMA((4,))],
        57, 1 << 30, 1 << 23, name="slots",
    )(expert_ids.T, out_proj, residual_in, gain)
    rows = experts * 8
    half = width // 2
    buf, carried = call(
        mix_kernel, (shape((rows, half), BF16), shape((tokens, width), F32)),
        [SM] + [VM] * 8, (VM, VM),
        [pltpu.VMEM((2 * tokens, half), BF16), pltpu.VMEM((rows, 2 * tokens), BF16)],
        24, 1 << 30, 1 << 23, name="mix",
    )(place, *parts, residual_v, proj_v, gain_v, tgt)
    arrived = lax.all_to_all(buf.reshape(experts, 8, half), ("sp", "tp"), split_axis=0, concat_axis=0, tiled=True)
    hidden = gate_proj.shape[2]
    result = call(
        expert_kernel, shape((rows, half), BF16), [VM] * 3 + [HB], VM,
        [
            pltpu.VMEM((hidden, width), BF16),
            pltpu.VMEM((rows // 2, width), BF16),
            pltpu.VMEM((rows // 2, hidden), BF16),
            pltpu.SemaphoreType.DMA((hidden // 256,)),
        ],
        40, 6 << 30, 1 << 24, name="experts",
    )(arrived.reshape(rows, half), gate_proj[0], up_proj[0], down_proj[0])
    returned = lax.all_to_all(result.reshape(experts, 8, half), ("sp", "tp"), split_axis=0, concat_axis=0, tiled=True)
    return call(
        combine_kernel, shape((tokens, width), BF16), [VM] * 4, VM,
        [pltpu.VMEM((2, 2 * tokens, rows), BF16)],
        12, 1 << 30, 1 << 22, name="combine",
    )(returned.reshape(rows, half), carried, tgt, expert_weights.T)


def solution(mesh):
    both = ("sp", "tp")
    in_specs = (
        P("sp", "tp"),
        P("sp", "tp"),
        P("sp", "tp"),
        P(None, "tp"),
        P("sp"),
        P(both, None),
        P(),
        P(),
        P(both, None),
        P(both, None),
        P(both, None, None),
        P(both, None, None),
        P(both, None, None),
    )
    return jax.shard_map(
        on_device, mesh=mesh, in_specs=in_specs, out_specs=P(both, None), check_vma=False
    )
```

```python
import functools
import jax
import jax.numpy as jnp
from jax import lax
from jax.experimental import pallas as pl
from jax.experimental.pallas import tpu as pltpu
from jax.sharding import PartitionSpec as P

F32 = jnp.float32
BF16 = jnp.bfloat16
EARLY = 62
SLOTS = 56
ORDER = (2, 1, 3)
VM = pl.BlockSpec(memory_space=pltpu.VMEM)
SM = pl.BlockSpec(memory_space=pltpu.SMEM)
HB = pl.BlockSpec(memory_space=pl.ANY)


def dot(a, b):
    return jnp.dot(a, b, preferred_element_type=F32)


def edge_kernel(x, g_in, docs, out, xv, gv, dv, sem):
    rows = x.shape[0]
    copies = [
        pltpu.make_async_copy(x.at[rows - 16 :, :], xv, sem.at[0]),
        pltpu.make_async_copy(g_in.at[rows - 16 :, :], gv, sem.at[1]),
        pltpu.make_async_copy(docs, dv, sem.at[2]),
    ]
    for copy in copies:
        copy.start()
    for copy in copies:
        copy.wait()
    prod = xv[...].astype(F32) * gv[...].astype(F32)
    last = dv.shape[0] - 1
    ids = jnp.broadcast_to(dv[last : last + 1, :].astype(F32), (128, 128)).T
    out[0:2, :] = prod[14:16, :]
    for c in range(out.shape[1] // 128):
        out[2:4, 128 * c : 128 * c + 128] = ids[126:128, :]


def taps_of(taps):
    return [taps[k : k + 1, :].astype(F32) for k in range(3)]


def conv_rows(window, ids, g_out, taps):
    count = window.shape[0] - 8
    cur = ids[8:]
    parts = []
    for half in range(window.shape[1] // 128):
        c = slice(128 * half, 128 * half + 128)
        back1 = jnp.where(ids[7:-1] == cur, window[7:-1, c], 0.0)
        back2 = jnp.where(ids[6:-2] == cur, window[6:-2, c], 0.0)
        mixed = taps[2][:, c] * window[8:, c] + taps[1][:, c] * back1 + taps[0][:, c] * back2
        parts.append((g_out[:, c].astype(F32) * mixed).astype(BF16))
    return parts


def slots_kernel(ids, proj, residual, gain, onehot, pick, proj_v, residual_v, gain_v, iv, sem):
    tokens = ids.shape[1]
    depth = proj.shape[0] // 4
    moves = [(ids, iv), (residual, residual_v), (gain, gain_v)]
    moves += [(proj.at[depth * j : depth * j + depth, :], proj_v.at[depth * j : depth * j + depth, :]) for j in range(4)]
    copies = [pltpu.make_async_copy(s, d, sem.at[i]) for i, (s, d) in enumerate(moves)]
    for copy in copies:
        copy.start()
    copies[0].wait()
    first = iv[0:1, :]
    second = iv[1:2, :]
    expert = lax.broadcasted_iota(jnp.int32, (128, tokens), 0)
    m0 = (expert == first).astype(F32)
    m1 = (expert == second).astype(F32)
    r = lax.broadcasted_iota(jnp.int32, (tokens, tokens), 0)
    c = lax.broadcasted_iota(jnp.int32, (tokens, tokens), 1)
    before = (r < c).astype(F32).astype(BF16)
    n0 = dot(m0.astype(BF16), before)
    n1 = dot(m1.astype(BF16), before) + jnp.sum(m0, axis=1, keepdims=True)
    rank0 = jnp.sum(m0 * n0, axis=0, keepdims=True).astype(jnp.int32)
    rank1 = jnp.sum(m1 * n1, axis=0, keepdims=True).astype(jnp.int32)
    target = [first * 8 + rank0, second * 8 + rank1]
    slots = onehot.shape[0]
    row = lax.broadcasted_iota(jnp.int32, (slots, tokens), 0)
    onehot[:, 0:tokens] = ((row == target[0]) | (row == target[1])).astype(F32).astype(BF16)
    onehot[:, tokens:] = ((row == target[0] + 4) | (row == target[1] + 4)).astype(F32).astype(BF16)
    for k in range(2):
        line = jnp.broadcast_to(target[k].astype(F32), (128, tokens)).T
        for n in range(slots // 128):
            lane = (lax.broadcasted_iota(jnp.int32, (tokens, 128), 1) + 128 * n).astype(F32)
            span = slice(128 * n, 128 * n + 128)
            pick[0, k * tokens : (k + 1) * tokens, span] = (line == lane).astype(F32).astype(BF16)
            pick[1, k * tokens : (k + 1) * tokens, span] = (line + 4.0 == lane).astype(F32).astype(BF16)
    for copy in copies[1:]:
        copy.wait()


def early_kernel(place, x, g_in, g_out, taps, docs, o0, o1, o2, o3, head, head_ids, gate_v, taps_v,
                 xv, gv, ov, dv, prod, doc_col, sem):
    rows = x.shape[0]
    part = o0.shape[0]
    moves = [(docs, dv), (taps, taps_v), (x, xv), (g_in, gv), (g_out, ov)]
    copies = [pltpu.make_async_copy(s, d, sem.at[i]) for i, (s, d) in enumerate(moves)]
    for copy in copies:
        copy.start()
    for copy in copies:
        copy.wait()
    prod[0:8, :] = jnp.zeros((8, x.shape[1]), F32)
    prod[8:, :] = xv[...].astype(F32) * gv[...].astype(F32)
    doc_col[0:8, :] = jnp.zeros((8, 128), F32)
    for block in range(rows // 128):
        line = jnp.broadcast_to(dv[block : block + 1, :].astype(F32), (128, 128))
        doc_col[8 + 128 * block : 136 + 128 * block, :] = line.T
    head[...] = prod[8:24, :]
    head_ids[...] = doc_col[8:24, :]
    gate_v[...] = ov[0:16, :]
    weights = taps_of(taps_v)
    here = place[0]
    for shift, out in enumerate((o0, o1, o2, o3)):
        start = pl.multiple_of(lax.rem(here + shift, 4) * part, part)
        pieces = conv_rows(
            prod[pl.ds(start, part + 8), :], doc_col[pl.ds(start, part + 8), :],
            ov[pl.ds(start, part), :], weights,
        )
        for half, piece in enumerate(pieces):
            out[:, 128 * half : 128 * half + 128] = piece


def fix_kernel(place, earlier, head, head_ids, g_out, taps, i0, i1, i2, i3, o0, o1, o2, o3):
    width = head.shape[1]
    here = place[0]
    window = jnp.concatenate([jnp.zeros((6, width), F32), earlier[0:2, :], head[...]], axis=0)
    ids = jnp.concatenate([jnp.zeros((6, 128), F32), earlier[2:4, 0:128], head_ids[...]], axis=0)
    pieces = conv_rows(window, ids, g_out[...], taps_of(taps))
    for shift, out in enumerate((o0, o1, o2, o3)):

        @pl.when(lax.rem(here + shift, 4) == 0)
        def _():
            for half, piece in enumerate(pieces):
                out[0:16, 128 * half : 128 * half + 128] = piece


def mix_kernel(place, r0, r1, r2, r3, residual, proj, gain, onehot, buf, carried, halves):
    here = place[0]
    width = residual.shape[1]
    half = width // 2
    tokens = residual.shape[0]
    step = 512
    total = jnp.zeros((tokens, 1), F32)
    for n in range(width // step):
        c = slice(n * step, n * step + step)
        acc = None
        for shift, part in enumerate((r0, r1, r2, r3)):
            depth = part.shape[1]
            start = pl.multiple_of(lax.rem(here + 4 - shift, 4) * depth, depth)
            term = dot(part[...], proj[pl.ds(start, depth), c])
            acc = term if acc is None else acc + term
        value = residual[:, c].astype(F32) + acc.astype(BF16).astype(F32)
        carried[:, c] = value
        total = total + jnp.sum(value * value, axis=1, keepdims=True)
    scale = lax.rsqrt(total * (1.0 / width) + 1e-06)
    for n in range(width // step):
        c = slice(n * step, n * step + step)
        value = (carried[:, c] * scale * gain[:, c]).astype(BF16)
        h = (n * step) // half
        halves[h * tokens : (h + 1) * tokens, n * step - h * half : n * step - h * half + step] = value
    for n in range(half // 256):
        c = slice(n * 256, n * 256 + 256)
        buf[:, c] = dot(onehot[...], halves[:, c]).astype(BF16)


def expert_kernel(arrived, wg, wu, wd, out, xv, hv):
    rows, half = arrived.shape
    blocks = wg.shape[1] // 256
    cols = [slice(256 * j, 256 * j + 256) for j in range(blocks)]
    low = lax.broadcasted_iota(jnp.int32, (rows // 16, 8, 256), 1) < 4
    for j, c in enumerate(cols):
        value = arrived[:, c].astype(F32).reshape(rows // 16, 2, 8, 256)
        even, odd = value[:, 0], value[:, 1]
        lo = jnp.where(low, even, pltpu.roll(odd, 4, 1))
        hi = jnp.where(low, pltpu.roll(even, 4, 1), odd)
        xv[:, c] = lo.reshape(rows // 2, 256).astype(BF16)
        xv[:, half + 256 * j : half + 256 * j + 256] = hi.reshape(rows // 2, 256).astype(BF16)
    for j, c in enumerate(cols):
        gate = dot(xv[...], wg[:, c])
        up = dot(xv[...], wu[:, c])
        hv[:, c] = (gate / (1.0 + jnp.exp(-gate)) * up).astype(BF16)
    for j, c in enumerate(cols):
        lo = dot(hv[...], wd[:, c]).reshape(rows // 16, 8, 256)
        hi = dot(hv[...], wd[:, half + 256 * j : half + 256 * j + 256]).reshape(rows // 16, 8, 256)
        even = jnp.where(low, lo, pltpu.roll(hi, 4, 1))
        odd = jnp.where(low, pltpu.roll(lo, 4, 1), hi)
        out[:, c] = jnp.stack([even, odd], axis=1).reshape(rows, 256).astype(BF16)


def combine_kernel(returned, carried, pick, weights, out, ov, sem):
    tokens = carried.shape[0]
    rows, half = returned.shape
    w = [jnp.broadcast_to(weights[k : k + 1, :], (128, tokens)).T[:, 0:1] for k in range(2)]
    copies = []
    for h in range(2):
        for n in range(half // 256):
            c = slice(256 * n, 256 * n + 256)
            d = slice(h * half + 256 * n, h * half + 256 * n + 256)
            both = dot(pick[h], returned[:, c])
            ov[:, d] = (carried[:, d] + (w[0] * both[:tokens] + w[1] * both[tokens:])).astype(BF16)
            copy = pltpu.make_async_copy(ov.at[:, d], out.at[:, d], sem.at[len(copies)])
            copy.start()
            copies.append(copy)
    for copy in copies:
        copy.wait()


def call(kernel, out_shape, in_specs, out_specs, scratch, vmem_mib, flops=0, nbytes=0, alias={}, name=None):
    return pl.pallas_call(
        kernel,
        out_shape=out_shape,
        in_specs=in_specs,
        out_specs=out_specs,
        scratch_shapes=scratch,
        input_output_aliases=alias,
        name=name,
        compiler_params=pltpu.CompilerParams(vmem_limit_bytes=int(vmem_mib * 1048576)),
        cost_estimate=pl.CostEstimate(flops=flops, bytes_accessed=nbytes, transcendentals=0),
    )


def shape(dims, kind):
    return jax.ShapeDtypeStruct(dims, kind)


def on_device(conv_input, gate_inner, gate_outer, conv_taps, doc_ids, residual_in, out_proj,
              norm_gain, expert_ids, expert_weights, gate_proj, up_proj, down_proj):
    length, channels = conv_input.shape
    tokens, width = residual_in.shape
    sp_count = lax.axis_size("sp")
    tp_count = lax.axis_size("tp")
    experts = sp_count * tp_count
    place = lax.axis_index("tp").reshape(1)
    docs = doc_ids.reshape(-1, 128)
    edge = call(
        edge_kernel, pltpu.VMEM((4, channels), F32), [HB] * 3, VM,
        [pltpu.VMEM((16, channels), BF16), pltpu.VMEM((16, channels), BF16),
         pltpu.VMEM(docs.shape, jnp.int32), pltpu.SemaphoreType.DMA((3,))],
        63, 1 << 20, 1 << 16, name="edge",
    )(conv_input, gate_inner, docs)
    earlier = lax.ppermute(edge, "sp", [(i, i + 1) for i in range(sp_count - 1)])
    gain = norm_gain.reshape(1, -1)
    rows = experts * 8
    half = width // 2
    piece = pltpu.VMEM((tokens, channels), BF16)
    outs = (piece,) * 4 + (
        pltpu.VMEM((16, channels), F32), pltpu.VMEM((16, 128), F32), pltpu.VMEM((16, channels), BF16),
        pltpu.VMEM(conv_taps.shape, BF16),
    )
    *raw, head, head_ids, gate_v, taps_v = call(
        early_kernel, outs, [SM] + [HB] * 5, (VM,) * len(outs),
        [
            pltpu.VMEM((length, channels), BF16), pltpu.VMEM((length, channels), BF16),
            pltpu.VMEM((length, channels), BF16), pltpu.VMEM(docs.shape, jnp.int32),
            pltpu.VMEM((length + 8, channels), F32),
            pltpu.VMEM((length + 8, 128), F32), pltpu.SemaphoreType.DMA((5,)),
        ],
        EARLY, 1 << 28, 1 << 20, name="early",
    )(place, conv_input, gate_inner, gate_outer, conv_taps, docs)
    sent = call(
        fix_kernel, (piece,) * 4, [SM] + [VM] * 9, (VM,) * 4, [], 4, 1 << 20, 1 << 18,
        alias={6 + k: k for k in range(4)}, name="fix",
    )(place, earlier, head, head_ids, gate_v, taps_v, *raw)
    parts = [sent[0], None, None, None]
    for d in ORDER:
        parts[d] = lax.ppermute(sent[d], "tp", [(i, (i + d) % tp_count) for i in range(tp_count)])
    held = (
        pltpu.VMEM((rows, 2 * tokens), BF16), pltpu.VMEM((2, 2 * tokens, rows), BF16),
        pltpu.VMEM(out_proj.shape, BF16), pltpu.VMEM(residual_in.shape, BF16), pltpu.VMEM(gain.shape, F32),
    )
    onehot, pick, proj_v, residual_v, gain_v = call(
        slots_kernel, held, [HB] * 4, (VM,) * 5,
        [pltpu.VMEM((2, tokens), jnp.int32), pltpu.SemaphoreType.DMA((7,))],
        SLOTS, 1 << 30, 1 << 23, name="slots",
    )(expert_ids.T, out_proj, residual_in, gain)
    buf, carried = call(
        mix_kernel, (shape((rows, half), BF16), shape((tokens, width), F32)),
        [SM] + [VM] * 8, (VM, VM),
        [pltpu.VMEM((2 * tokens, half), BF16)],
        12, 8 << 30, 1 << 23, name="mix",
    )(place, *parts, residual_v, proj_v, gain_v, onehot)
    arrived = lax.all_to_all(buf.reshape(experts, 8, half), ("sp", "tp"), split_axis=0, concat_axis=0, tiled=True)
    hidden = gate_proj.shape[2]
    result = call(
        expert_kernel, shape((rows, half), BF16), [VM] * 4, VM,
        [
            pltpu.VMEM((rows // 2, width), BF16),
            pltpu.VMEM((rows // 2, hidden), BF16),
        ],
        20, 6 << 30, 1 << 24, name="experts",
    )(arrived.reshape(rows, half), gate_proj[0], up_proj[0], down_proj[0])
    returned = lax.all_to_all(result.reshape(experts, 8, half), ("sp", "tp"), split_axis=0, concat_axis=0, tiled=True)
    return call(
        combine_kernel, shape((tokens, width), BF16), [VM] * 4, HB,
        [pltpu.VMEM((tokens, width), BF16), pltpu.SemaphoreType.DMA((8,))],
        12, 1 << 30, 1 << 22, name="combine",
    )(returned.reshape(rows, half), carried, pick, expert_weights.T)


def solution(mesh):
    both = ("sp", "tp")
    in_specs = (
        P("sp", "tp"),
        P("sp", "tp"),
        P("sp", "tp"),
        P(None, "tp"),
        P("sp"),
        P(both, None),
        P(),
        P(),
        P(both, None),
        P(both, None),
        P(both, None, None),
        P(both, None, None),
        P(both, None, None),
    )
    return jax.shard_map(
        on_device, mesh=mesh, in_specs=in_specs, out_specs=P(both, None), check_vma=False
    )
```

```python
import functools
import jax
import jax.numpy as jnp
from jax import lax
from jax.experimental import pallas as pl
from jax.experimental.pallas import tpu as pltpu
from jax.sharding import PartitionSpec as P

F32 = jnp.float32
BF16 = jnp.bfloat16
EDGE = 61
EARLY = 24
SLOTS = 8
SLOT_FLOPS = 2 << 30
EARLY_FLOPS = 8 << 30
EDGE_FLOPS = 8 << 30
ORDER = (2, 1, 3)
VM = pl.BlockSpec(memory_space=pltpu.VMEM)
SM = pl.BlockSpec(memory_space=pltpu.SMEM)
HB = pl.BlockSpec(memory_space=pl.ANY)


def dot(a, b):
    return jnp.dot(a, b, preferred_element_type=F32)


def edge_kernel(x, g_in, docs, out, xv, gv, dv, sem):
    rows = x.shape[0]
    copies = [
        pltpu.make_async_copy(x.at[rows - 16 :, :], xv, sem.at[0]),
        pltpu.make_async_copy(g_in.at[rows - 16 :, :], gv, sem.at[1]),
        pltpu.make_async_copy(docs, dv, sem.at[2]),
    ]
    for copy in copies:
        copy.start()
    for copy in copies:
        copy.wait()
    prod = xv[...].astype(F32) * gv[...].astype(F32)
    last = dv.shape[0] - 1
    ids = jnp.broadcast_to(dv[last : last + 1, :].astype(F32), (128, 128)).T
    out[0:2, :] = prod[14:16, :]
    for c in range(out.shape[1] // 128):
        out[2:4, 128 * c : 128 * c + 128] = ids[126:128, :]


def taps_of(taps):
    return [taps[k : k + 1, :].astype(F32) for k in range(3)]


def conv_rows(window, ids, g_out, taps):
    count = window.shape[0] - 8
    cur = ids[8:]
    parts = []
    for half in range(window.shape[1] // 128):
        c = slice(128 * half, 128 * half + 128)
        back1 = jnp.where(ids[7:-1] == cur, window[7:-1, c], 0.0)
        back2 = jnp.where(ids[6:-2] == cur, window[6:-2, c], 0.0)
        mixed = taps[2][:, c] * window[8:, c] + taps[1][:, c] * back1 + taps[0][:, c] * back2
        parts.append((g_out[:, c].astype(F32) * mixed).astype(BF16))
    return parts


def slots_kernel(iv, onehot, pick):
    tokens = iv.shape[1]
    first = iv[0:1, :]
    second = iv[1:2, :]
    expert = lax.broadcasted_iota(jnp.int32, (128, tokens), 0)
    m0 = (expert == first).astype(F32)
    m1 = (expert == second).astype(F32)
    r = lax.broadcasted_iota(jnp.int32, (tokens, tokens), 0)
    c = lax.broadcasted_iota(jnp.int32, (tokens, tokens), 1)
    before = (r < c).astype(F32).astype(BF16)
    n0 = dot(m0.astype(BF16), before)
    n1 = dot(m1.astype(BF16), before) + jnp.sum(m0, axis=1, keepdims=True)
    rank0 = jnp.sum(m0 * n0, axis=0, keepdims=True).astype(jnp.int32)
    rank1 = jnp.sum(m1 * n1, axis=0, keepdims=True).astype(jnp.int32)
    target = [first * 8 + rank0, second * 8 + rank1]
    slots = onehot.shape[0]
    row = lax.broadcasted_iota(jnp.int32, (slots, tokens), 0)
    onehot[:, 0:tokens] = ((row == target[0]) | (row == target[1])).astype(F32).astype(BF16)
    onehot[:, tokens:] = ((row == target[0] + 4) | (row == target[1] + 4)).astype(F32).astype(BF16)
    for k, (chosen, rank) in enumerate(((first, rank0), (second, rank1))):
        line = jnp.broadcast_to((chosen * 4 + rank).astype(F32), (128, tokens)).T
        for n in range(pick.shape[1] // 128):
            lane = (lax.broadcasted_iota(jnp.int32, (tokens, 128), 1) + 128 * n).astype(F32)
            span = slice(128 * n, 128 * n + 128)
            pick[k * tokens : (k + 1) * tokens, span] = (line == lane).astype(F32).astype(BF16)


def early_kernel(place, xv, gv, ov, taps, dv, o0, o1, o2, o3, head, head_ids, gate_v, taps_v, prod, doc_col):
    rows = xv.shape[0]
    part = o0.shape[0]
    taps_v[...] = taps[...]
    prod[0:8, :] = jnp.zeros((8, xv.shape[1]), F32)
    prod[8:, :] = xv[...].astype(F32) * gv[...].astype(F32)
    doc_col[0:8, :] = jnp.zeros((8, 128), F32)
    for block in range(rows // 128):
        line = jnp.broadcast_to(dv[block : block + 1, :].astype(F32), (128, 128))
        doc_col[8 + 128 * block : 136 + 128 * block, :] = line.T
    head[...] = prod[8:24, :]
    head_ids[...] = doc_col[8:24, :]
    gate_v[...] = ov[0:16, :]
    weights = taps_of(taps_v)
    here = place[0]
    for shift, out in enumerate((o0, o1, o2, o3)):
        start = pl.multiple_of(lax.rem(here + shift, 4) * part, part)
        pieces = conv_rows(
            prod[pl.ds(start, part + 8), :], doc_col[pl.ds(start, part + 8), :],
            ov[pl.ds(start, part), :], weights,
        )
        for half, piece in enumerate(pieces):
            out[:, 128 * half : 128 * half + 128] = piece


def fix_kernel(place, earlier, head, head_ids, g_out, taps, i0, i1, i2, i3, o0, o1, o2, o3):
    width = head.shape[1]
    part = i0.shape[0]
    here = place[0]
    window = jnp.concatenate([jnp.zeros((6, width), F32), earlier[0:2, :], head[...]], axis=0)
    ids = jnp.concatenate([jnp.zeros((6, 128), F32), earlier[2:4, 0:128], head_ids[...]], axis=0)
    pieces = conv_rows(window, ids, g_out[...], taps_of(taps))
    for shift, (old, out) in enumerate(zip((i0, i1, i2, i3), (o0, o1, o2, o3))):
        out[16:part, :] = old[16:part, :]
        mine = jnp.full((16, 128), lax.rem(here + shift, 4), jnp.int32) == 0
        for half, piece in enumerate(pieces):
            c = slice(128 * half, 128 * half + 128)
            out[0:16, c] = jnp.where(mine, piece.astype(F32), old[0:16, c].astype(F32)).astype(BF16)


def mix_kernel(place, r0, r1, r2, r3, residual, proj, gain, onehot, buf, carried, halves):
    here = place[0]
    width = residual.shape[1]
    half = width // 2
    tokens = residual.shape[0]
    step = 512
    total = jnp.zeros((tokens, 1), F32)
    for n in range(width // step):
        c = slice(n * step, n * step + step)
        acc = None
        for shift, part in enumerate((r0, r1, r2, r3)):
            depth = part.shape[1]
            start = pl.multiple_of(lax.rem(here + 4 - shift, 4) * depth, depth)
            term = dot(part[...], proj[pl.ds(start, depth), c])
            acc = term if acc is None else acc + term
        value = residual[:, c].astype(F32) + acc.astype(BF16).astype(F32)
        carried[:, c] = value
        total = total + jnp.sum(value * value, axis=1, keepdims=True)
    scale = lax.rsqrt(total * (1.0 / width) + 1e-06)
    for n in range(width // step):
        c = slice(n * step, n * step + step)
        value = (carried[:, c] * scale * gain[:, c]).astype(BF16)
        h = (n * step) // half
        halves[h * tokens : (h + 1) * tokens, n * step - h * half : n * step - h * half + step] = value
    for n in range(half // 256):
        c = slice(n * 256, n * 256 + 256)
        buf[:, c] = dot(onehot[...], halves[:, c]).astype(BF16)


def expert_kernel(arrived, wg, wu, wd, out, xv, hv):
    rows, half = arrived.shape
    blocks = wg.shape[1] // 256
    cols = [slice(256 * j, 256 * j + 256) for j in range(blocks)]
    low = lax.broadcasted_iota(jnp.int32, (rows // 16, 8, 256), 1) < 4
    for j, c in enumerate(cols):
        value = arrived[:, c].astype(F32).reshape(rows // 16, 2, 8, 256)
        even, odd = value[:, 0], value[:, 1]
        lo = jnp.where(low, even, pltpu.roll(odd, 4, 1))
        hi = jnp.where(low, pltpu.roll(even, 4, 1), odd)
        xv[:, c] = lo.reshape(rows // 2, 256).astype(BF16)
        xv[:, half + 256 * j : half + 256 * j + 256] = hi.reshape(rows // 2, 256).astype(BF16)
    for j, c in enumerate(cols):
        gate = dot(xv[...], wg[:, c])
        up = dot(xv[...], wu[:, c])
        hv[:, c] = (gate / (1.0 + jnp.exp(-gate)) * up).astype(BF16)
    for j, c in enumerate(cols):
        lo = dot(hv[...], wd[:, c]).reshape(rows // 16, 8, 256)
        hi = dot(hv[...], wd[:, half + 256 * j : half + 256 * j + 256]).reshape(rows // 16, 8, 256)
        even = jnp.where(low, lo, pltpu.roll(hi, 4, 1))
        odd = jnp.where(low, pltpu.roll(lo, 4, 1), hi)
        out[:, c] = jnp.stack([even, odd], axis=1).reshape(rows, 256).astype(BF16)


def combine_kernel(returned, carried, pick, weights, out, ov, sem):
    tokens = carried.shape[0]
    rows, half = returned.shape
    w = [jnp.broadcast_to(weights[k : k + 1, :], (128, tokens)).T[:, 0:1] for k in range(2)]
    low = lax.broadcasted_iota(jnp.int32, (rows // 16, 8, 256), 1) < 4
    copies = []
    for n in range(half // 256):
        c = slice(256 * n, 256 * n + 256)
        value = returned[:, c].astype(F32).reshape(rows // 16, 2, 8, 256)
        even, odd = value[:, 0], value[:, 1]
        lo = jnp.where(low, even, pltpu.roll(odd, 4, 1))
        hi = jnp.where(low, pltpu.roll(even, 4, 1), odd)
        for h, source in enumerate((lo, hi)):
            d = slice(h * half + 256 * n, h * half + 256 * n + 256)
            both = dot(pick[...], source.reshape(rows // 2, 256).astype(BF16))
            ov[:, d] = (carried[:, d] + (w[0] * both[:tokens] + w[1] * both[tokens:])).astype(BF16)
            copy = pltpu.make_async_copy(ov.at[:, d], out.at[:, d], sem.at[len(copies)])
            copy.start()
            copies.append(copy)
    for copy in copies:
        copy.wait()


def call(kernel, out_shape, in_specs, out_specs, scratch, vmem_mib, flops=0, nbytes=0, name=None):
    return pl.pallas_call(
        kernel,
        out_shape=out_shape,
        in_specs=in_specs,
        out_specs=out_specs,
        scratch_shapes=scratch,
        name=name,
        compiler_params=pltpu.CompilerParams(vmem_limit_bytes=int(vmem_mib * 1048576)),
        cost_estimate=pl.CostEstimate(flops=flops, bytes_accessed=nbytes, transcendentals=0),
    )


def shape(dims, kind):
    return jax.ShapeDtypeStruct(dims, kind)


def on_device(conv_input, gate_inner, gate_outer, conv_taps, doc_ids, residual_in, out_proj,
              norm_gain, expert_ids, expert_weights, gate_proj, up_proj, down_proj):
    length, channels = conv_input.shape
    tokens, width = residual_in.shape
    sp_count = lax.axis_size("sp")
    tp_count = lax.axis_size("tp")
    experts = sp_count * tp_count
    place = lax.axis_index("tp").reshape(1)
    docs = doc_ids.reshape(-1, 128)
    edge = call(
        edge_kernel, pltpu.VMEM((4, channels), F32), [HB] * 3, VM,
        [pltpu.VMEM((16, channels), BF16), pltpu.VMEM((16, channels), BF16),
         pltpu.VMEM(docs.shape, jnp.int32), pltpu.SemaphoreType.DMA((3,))],
        EDGE, EDGE_FLOPS, 1 << 16, name="edge",
    )(conv_input, gate_inner, docs)
    earlier = lax.ppermute(edge, "sp", [(i, i + 1) for i in range(sp_count - 1)])
    gain = norm_gain.reshape(1, -1)
    rows = experts * 8
    half = width // 2
    piece = pltpu.VMEM((tokens, channels), BF16)
    outs = (piece,) * 4 + (
        pltpu.VMEM((16, channels), F32), pltpu.VMEM((16, 128), F32), pltpu.VMEM((16, channels), BF16),
        pltpu.VMEM(conv_taps.shape, BF16),
    )
    *raw, head, head_ids, gate_v, taps_v = call(
        early_kernel, outs, [SM] + [VM] * 5, (VM,) * len(outs),
        [pltpu.VMEM((length + 8, channels), F32), pltpu.VMEM((length + 8, 128), F32)],
        EARLY, EARLY_FLOPS, 1 << 20, name="early",
    )(place, conv_input, gate_inner, gate_outer, conv_taps, docs)
    sent = call(
        fix_kernel, (piece,) * 4, [SM] + [VM] * 9, (VM,) * 4, [], 4, 1 << 20, 1 << 18,
        name="fix",
    )(place, earlier, head, head_ids, gate_v, taps_v, *raw)
    parts = [sent[0], None, None, None]
    for d in ORDER:
        parts[d] = lax.ppermute(sent[d], "tp", [(i, (i + d) % tp_count) for i in range(tp_count)])
    held = (pltpu.VMEM((rows, 2 * tokens), BF16), pltpu.VMEM((2 * tokens, rows // 2), BF16))
    onehot, pick = call(
        slots_kernel, held, [VM], (VM,) * 2, [], SLOTS, SLOT_FLOPS, 1 << 20, name="slots",
    )(expert_ids.T)
    buf, carried = call(
        mix_kernel, (shape((rows, half), BF16), shape((tokens, width), F32)),
        [SM] + [VM] * 8, (VM, VM),
        [pltpu.VMEM((2 * tokens, half), BF16)],
        12, 8 << 30, 1 << 23, name="mix",
    )(place, *parts, residual_in, out_proj, gain, onehot)
    arrived = lax.all_to_all(buf.reshape(experts, 8, half), ("sp", "tp"), split_axis=0, concat_axis=0, tiled=True)
    hidden = gate_proj.shape[2]
    result = call(
        expert_kernel, shape((rows, half), BF16), [VM] * 4, VM,
        [
            pltpu.VMEM((rows // 2, width), BF16),
            pltpu.VMEM((rows // 2, hidden), BF16),
        ],
        20, 6 << 30, 1 << 24, name="experts",
    )(arrived.reshape(rows, half), gate_proj[0], up_proj[0], down_proj[0])
    returned = lax.all_to_all(result.reshape(experts, 8, half), ("sp", "tp"), split_axis=0, concat_axis=0, tiled=True)
    return call(
        combine_kernel, shape((tokens, width), BF16), [VM] * 4, HB,
        [pltpu.VMEM((tokens, width), BF16), pltpu.SemaphoreType.DMA((8,))],
        12, 1 << 30, 1 << 22, name="combine",
    )(returned.reshape(rows, half), carried, pick, expert_weights.T)


def solution(mesh):
    both = ("sp", "tp")
    in_specs = (
        P("sp", "tp"),
        P("sp", "tp"),
        P("sp", "tp"),
        P(None, "tp"),
        P("sp"),
        P(both, None),
        P(),
        P(),
        P(both, None),
        P(both, None),
        P(both, None, None),
        P(both, None, None),
        P(both, None, None),
    )
    return jax.shard_map(
        on_device, mesh=mesh, in_specs=in_specs, out_specs=P(both, None), check_vma=False
    )
```

```python
import functools
import jax
import jax.numpy as jnp
from jax import lax
from jax.experimental import pallas as pl
from jax.experimental.pallas import tpu as pltpu
from jax.sharding import PartitionSpec as P

F32 = jnp.float32
BF16 = jnp.bfloat16
EDGE = 61
EARLY = 24
SLOTS = 8
SLOT_FLOPS = 2 << 30
EARLY_FLOPS = 8 << 30
EDGE_FLOPS = 8 << 30
ORDER = (2, 1, 3)
VM = pl.BlockSpec(memory_space=pltpu.VMEM)
SM = pl.BlockSpec(memory_space=pltpu.SMEM)
HB = pl.BlockSpec(memory_space=pl.ANY)


def dot(a, b):
    return jnp.dot(a, b, preferred_element_type=F32)


def edge_kernel(x, g_in, docs, out, xv, gv, dv, sem):
    rows = x.shape[0]
    copies = [
        pltpu.make_async_copy(x.at[rows - 16 :, :], xv, sem.at[0]),
        pltpu.make_async_copy(g_in.at[rows - 16 :, :], gv, sem.at[1]),
        pltpu.make_async_copy(docs, dv, sem.at[2]),
    ]
    for copy in copies:
        copy.start()
    for copy in copies:
        copy.wait()
    prod = xv[...].astype(F32) * gv[...].astype(F32)
    last = dv.shape[0] - 1
    out[0:2, :] = prod[14:16, :]
    for c in range(out.shape[1] // 128):
        out[2:4, 128 * c : 128 * c + 128] = jnp.broadcast_to(dv[last : last + 1, :].astype(F32), (2, 128))


def taps_of(taps):
    return [taps[k : k + 1, :].astype(F32) for k in range(3)]


def conv_rows(window, ids, g_out, taps):
    count = window.shape[0] - 8
    cur = ids[8:]
    parts = []
    for half in range(window.shape[1] // 128):
        c = slice(128 * half, 128 * half + 128)
        back1 = jnp.where(ids[7:-1] == cur, window[7:-1, c], 0.0)
        back2 = jnp.where(ids[6:-2] == cur, window[6:-2, c], 0.0)
        mixed = taps[2][:, c] * window[8:, c] + taps[1][:, c] * back1 + taps[0][:, c] * back2
        parts.append((g_out[:, c].astype(F32) * mixed).astype(BF16))
    return parts


def slots_kernel(iv, onehot, pick):
    tokens = iv.shape[1]
    first = iv[0:1, :]
    second = iv[1:2, :]
    expert = lax.broadcasted_iota(jnp.int32, (128, tokens), 0)
    m0 = (expert == first).astype(F32)
    m1 = (expert == second).astype(F32)
    r = lax.broadcasted_iota(jnp.int32, (tokens, tokens), 0)
    c = lax.broadcasted_iota(jnp.int32, (tokens, tokens), 1)
    before = (r < c).astype(F32).astype(BF16)
    n0 = dot(m0.astype(BF16), before)
    n1 = dot(m1.astype(BF16), before) + jnp.sum(m0, axis=1, keepdims=True)
    rank0 = jnp.sum(m0 * n0, axis=0, keepdims=True).astype(jnp.int32)
    rank1 = jnp.sum(m1 * n1, axis=0, keepdims=True).astype(jnp.int32)
    target = [first * 8 + rank0, second * 8 + rank1]
    slots = onehot.shape[0]
    row = lax.broadcasted_iota(jnp.int32, (slots, tokens), 0)
    onehot[:, 0:tokens] = ((row == target[0]) | (row == target[1])).astype(F32).astype(BF16)
    onehot[:, tokens:] = ((row == target[0] + 4) | (row == target[1] + 4)).astype(F32).astype(BF16)
    for k, (chosen, rank) in enumerate(((first, rank0), (second, rank1))):
        line = jnp.broadcast_to((chosen * 4 + rank).astype(F32), (128, tokens)).T
        for n in range(pick.shape[1] // 128):
            lane = (lax.broadcasted_iota(jnp.int32, (tokens, 128), 1) + 128 * n).astype(F32)
            span = slice(128 * n, 128 * n + 128)
            pick[k * tokens : (k + 1) * tokens, span] = (line == lane).astype(F32).astype(BF16)


def early_kernel(place, xv, gv, ov, taps, dv, o0, o1, o2, o3, head, head_ids, gate_v, taps_v, prod, doc_col):
    rows = xv.shape[0]
    part = o0.shape[0]
    taps_v[...] = taps[...]
    prod[0:8, :] = jnp.zeros((8, xv.shape[1]), F32)
    prod[8:, :] = xv[...].astype(F32) * gv[...].astype(F32)
    doc_col[0:8, :] = jnp.zeros((8, 128), F32)
    for block in range(rows // 128):
        line = jnp.broadcast_to(dv[block : block + 1, :].astype(F32), (128, 128))
        doc_col[8 + 128 * block : 136 + 128 * block, :] = line.T
    head[...] = prod[8:24, :]
    head_ids[...] = doc_col[8:24, :]
    gate_v[...] = ov[0:16, :]
    weights = taps_of(taps_v)
    here = place[0]
    for shift, out in enumerate((o0, o1, o2, o3)):
        start = pl.multiple_of(lax.rem(here + shift, 4) * part, part)
        pieces = conv_rows(
            prod[pl.ds(start, part + 8), :], doc_col[pl.ds(start, part + 8), :],
            ov[pl.ds(start, part), :], weights,
        )
        for half, piece in enumerate(pieces):
            out[:, 128 * half : 128 * half + 128] = piece


def fix_kernel(place, earlier, head, head_ids, g_out, taps, i0, i1, i2, i3, o0, o1, o2, o3):
    width = head.shape[1]
    part = i0.shape[0]
    here = place[0]
    window = jnp.concatenate([jnp.zeros((6, width), F32), earlier[0:2, :], head[...]], axis=0)
    before = [jnp.broadcast_to(earlier[2:3, k : k + 1], (1, 128)) for k in (126, 127)]
    ids = jnp.concatenate([jnp.zeros((6, 128), F32), *before, head_ids[...]], axis=0)
    pieces = conv_rows(window, ids, g_out[...], taps_of(taps))
    for shift, (old, out) in enumerate(zip((i0, i1, i2, i3), (o0, o1, o2, o3))):
        out[16:part, :] = old[16:part, :]
        mine = jnp.full((16, 128), lax.rem(here + shift, 4), jnp.int32) == 0
        for half, piece in enumerate(pieces):
            c = slice(128 * half, 128 * half + 128)
            out[0:16, c] = jnp.where(mine, piece.astype(F32), old[0:16, c].astype(F32)).astype(BF16)


def mix_kernel(place, r0, r1, r2, r3, residual, proj, gain, onehot, buf, carried, halves):
    here = place[0]
    width = residual.shape[1]
    half = width // 2
    tokens = residual.shape[0]
    step = 512
    total = jnp.zeros((tokens, 1), F32)
    for n in range(width // step):
        c = slice(n * step, n * step + step)
        acc = None
        for shift, part in enumerate((r0, r1, r2, r3)):
            depth = part.shape[1]
            start = pl.multiple_of(lax.rem(here + 4 - shift, 4) * depth, depth)
            term = dot(part[...], proj[pl.ds(start, depth), c])
            acc = term if acc is None else acc + term
        value = residual[:, c].astype(F32) + acc.astype(BF16).astype(F32)
        carried[:, c] = value
        total = total + jnp.sum(value * value, axis=1, keepdims=True)
    scale = lax.rsqrt(total * (1.0 / width) + 1e-06)
    for n in range(width // step):
        c = slice(n * step, n * step + step)
        value = (carried[:, c] * scale * gain[:, c]).astype(BF16)
        h = (n * step) // half
        halves[h * tokens : (h + 1) * tokens, n * step - h * half : n * step - h * half + step] = value
    for n in range(half // 256):
        c = slice(n * 256, n * 256 + 256)
        buf[:, c] = dot(onehot[...], halves[:, c]).astype(BF16)


def expert_kernel(arrived, wg, wu, wd, out, xv, hv):
    rows, half = arrived.shape
    blocks = wg.shape[1] // 256
    cols = [slice(256 * j, 256 * j + 256) for j in range(blocks)]
    low = lax.broadcasted_iota(jnp.int32, (rows // 16, 8, 256), 1) < 4
    for j, c in enumerate(cols):
        value = arrived[:, c].astype(F32).reshape(rows // 16, 2, 8, 256)
        even, odd = value[:, 0], value[:, 1]
        lo = jnp.where(low, even, pltpu.roll(odd, 4, 1))
        hi = jnp.where(low, pltpu.roll(even, 4, 1), odd)
        xv[:, c] = lo.reshape(rows // 2, 256).astype(BF16)
        xv[:, half + 256 * j : half + 256 * j + 256] = hi.reshape(rows // 2, 256).astype(BF16)
    for j, c in enumerate(cols):
        gate = dot(xv[...], wg[:, c])
        up = dot(xv[...], wu[:, c])
        hv[:, c] = (gate / (1.0 + jnp.exp(-gate)) * up).astype(BF16)
    for j, c in enumerate(cols):
        lo = dot(hv[...], wd[:, c]).reshape(rows // 16, 8, 256)
        hi = dot(hv[...], wd[:, half + 256 * j : half + 256 * j + 256]).reshape(rows // 16, 8, 256)
        even = jnp.where(low, lo, pltpu.roll(hi, 4, 1))
        odd = jnp.where(low, pltpu.roll(lo, 4, 1), hi)
        out[:, c] = jnp.stack([even, odd], axis=1).reshape(rows, 256).astype(BF16)


def combine_kernel(returned, carried, pick, weights, out, ov, sem):
    tokens = carried.shape[0]
    rows, half = returned.shape
    w = [jnp.broadcast_to(weights[k : k + 1, :], (128, tokens)).T[:, 0:1] for k in range(2)]
    low = lax.broadcasted_iota(jnp.int32, (rows // 16, 8, 256), 1) < 4
    copies = []
    for n in range(half // 256):
        c = slice(256 * n, 256 * n + 256)
        value = returned[:, c].astype(F32).reshape(rows // 16, 2, 8, 256)
        even, odd = value[:, 0], value[:, 1]
        lo = jnp.where(low, even, pltpu.roll(odd, 4, 1))
        hi = jnp.where(low, pltpu.roll(even, 4, 1), odd)
        for h, source in enumerate((lo, hi)):
            d = slice(h * half + 256 * n, h * half + 256 * n + 256)
            both = dot(pick[...], source.reshape(rows // 2, 256).astype(BF16))
            ov[:, d] = (carried[:, d] + (w[0] * both[:tokens] + w[1] * both[tokens:])).astype(BF16)
            copy = pltpu.make_async_copy(ov.at[:, d], out.at[:, d], sem.at[len(copies)])
            copy.start()
            copies.append(copy)
    for copy in copies:
        copy.wait()


def call(kernel, out_shape, in_specs, out_specs, scratch, vmem_mib, flops=0, nbytes=0, name=None):
    return pl.pallas_call(
        kernel,
        out_shape=out_shape,
        in_specs=in_specs,
        out_specs=out_specs,
        scratch_shapes=scratch,
        name=name,
        compiler_params=pltpu.CompilerParams(vmem_limit_bytes=int(vmem_mib * 1048576)),
        cost_estimate=pl.CostEstimate(flops=flops, bytes_accessed=nbytes, transcendentals=0),
    )


def shape(dims, kind):
    return jax.ShapeDtypeStruct(dims, kind)


def on_device(conv_input, gate_inner, gate_outer, conv_taps, doc_ids, residual_in, out_proj,
              norm_gain, expert_ids, expert_weights, gate_proj, up_proj, down_proj):
    length, channels = conv_input.shape
    tokens, width = residual_in.shape
    sp_count = lax.axis_size("sp")
    tp_count = lax.axis_size("tp")
    experts = sp_count * tp_count
    place = lax.axis_index("tp").reshape(1)
    docs = doc_ids.reshape(-1, 128)
    edge = call(
        edge_kernel, pltpu.VMEM((4, channels), F32), [HB] * 3, VM,
        [pltpu.VMEM((16, channels), BF16), pltpu.VMEM((16, channels), BF16),
         pltpu.VMEM(docs.shape, jnp.int32), pltpu.SemaphoreType.DMA((3,))],
        EDGE, EDGE_FLOPS, 1 << 16, name="edge",
    )(conv_input, gate_inner, docs)
    earlier = lax.ppermute(edge, "sp", [(i, i + 1) for i in range(sp_count - 1)])
    gain = norm_gain.reshape(1, -1)
    rows = experts * 8
    half = width // 2
    piece = pltpu.VMEM((tokens, channels), BF16)
    outs = (piece,) * 4 + (
        pltpu.VMEM((16, channels), F32), pltpu.VMEM((16, 128), F32), pltpu.VMEM((16, channels), BF16),
        pltpu.VMEM(conv_taps.shape, BF16),
    )
    *raw, head, head_ids, gate_v, taps_v = call(
        early_kernel, outs, [SM] + [VM] * 5, (VM,) * len(outs),
        [pltpu.VMEM((length + 8, channels), F32), pltpu.VMEM((length + 8, 128), F32)],
        EARLY, EARLY_FLOPS, 1 << 20, name="early",
    )(place, conv_input, gate_inner, gate_outer, conv_taps, docs)
    sent = call(
        fix_kernel, (piece,) * 4, [SM] + [VM] * 9, (VM,) * 4, [], 4, 1 << 20, 1 << 18,
        name="fix",
    )(place, earlier, head, head_ids, gate_v, taps_v, *raw)
    parts = [sent[0], None, None, None]
    for d in ORDER:
        parts[d] = lax.ppermute(sent[d], "tp", [(i, (i + d) % tp_count) for i in range(tp_count)])
    held = (pltpu.VMEM((rows, 2 * tokens), BF16), pltpu.VMEM((2 * tokens, rows // 2), BF16))
    onehot, pick = call(
        slots_kernel, held, [VM], (VM,) * 2, [], SLOTS, SLOT_FLOPS, 1 << 20, name="slots",
    )(expert_ids.T)
    buf, carried = call(
        mix_kernel, (shape((rows, half), BF16), shape((tokens, width), F32)),
        [SM] + [VM] * 8, (VM, VM),
        [pltpu.VMEM((2 * tokens, half), BF16)],
        12, 8 << 30, 1 << 23, name="mix",
    )(place, *parts, residual_in, out_proj, gain, onehot)
    arrived = lax.all_to_all(buf.reshape(experts, 8, half), ("sp", "tp"), split_axis=0, concat_axis=0, tiled=True)
    hidden = gate_proj.shape[2]
    result = call(
        expert_kernel, shape((rows, half), BF16), [VM] * 4, VM,
        [
            pltpu.VMEM((rows // 2, width), BF16),
            pltpu.VMEM((rows // 2, hidden), BF16),
        ],
        20, 6 << 30, 1 << 24, name="experts",
    )(arrived.reshape(rows, half), gate_proj[0], up_proj[0], down_proj[0])
    returned = lax.all_to_all(result.reshape(experts, 8, half), ("sp", "tp"), split_axis=0, concat_axis=0, tiled=True)
    return call(
        combine_kernel, shape((tokens, width), BF16), [VM] * 4, HB,
        [pltpu.VMEM((tokens, width), BF16), pltpu.SemaphoreType.DMA((8,))],
        12, 1 << 30, 1 << 22, name="combine",
    )(returned.reshape(rows, half), carried, pick, expert_weights.T)


def solution(mesh):
    both = ("sp", "tp")
    in_specs = (
        P("sp", "tp"),
        P("sp", "tp"),
        P("sp", "tp"),
        P(None, "tp"),
        P("sp"),
        P(both, None),
        P(),
        P(),
        P(both, None),
        P(both, None),
        P(both, None, None),
        P(both, None, None),
        P(both, None, None),
    )
    return jax.shard_map(
        on_device, mesh=mesh, in_specs=in_specs, out_specs=P(both, None), check_vma=False
    )
```

```python
import functools
import jax
import jax.numpy as jnp
from jax import lax
from jax.experimental import pallas as pl
from jax.experimental.pallas import tpu as pltpu
from jax.sharding import PartitionSpec as P

F32 = jnp.float32
BF16 = jnp.bfloat16
EDGE = 61
EARLY = 24
SLOTS = 8
SLOT_FLOPS = 2 << 30
EARLY_FLOPS = 8 << 30
EDGE_FLOPS = 8 << 30
ORDER = (2, 1, 3)
VM = pl.BlockSpec(memory_space=pltpu.VMEM)
SM = pl.BlockSpec(memory_space=pltpu.SMEM)
HB = pl.BlockSpec(memory_space=pl.ANY)


def dot(a, b):
    return jnp.dot(a, b, preferred_element_type=F32)


def edge_kernel(x, g_in, docs, out, xv, gv, dv, sem):
    rows = x.shape[0]
    copies = [
        pltpu.make_async_copy(x.at[rows - 16 :, :], xv, sem.at[0]),
        pltpu.make_async_copy(g_in.at[rows - 16 :, :], gv, sem.at[1]),
        pltpu.make_async_copy(docs, dv, sem.at[2]),
    ]
    for copy in copies:
        copy.start()
    for copy in copies:
        copy.wait()
    prod = xv[...].astype(F32) * gv[...].astype(F32)
    last = dv.shape[0] - 1
    out[0:2, :] = prod[14:16, :]
    for c in range(out.shape[1] // 128):
        out[2:4, 128 * c : 128 * c + 128] = jnp.broadcast_to(dv[last : last + 1, :].astype(F32), (2, 128))


def taps_of(taps):
    return [taps[k : k + 1, :].astype(F32) for k in range(3)]


def conv_rows(window, ids, g_out, taps):
    count = window.shape[0] - 8
    cur = ids[8:]
    parts = []
    for half in range(window.shape[1] // 128):
        c = slice(128 * half, 128 * half + 128)
        back1 = jnp.where(ids[7:-1] == cur, window[7:-1, c], 0.0)
        back2 = jnp.where(ids[6:-2] == cur, window[6:-2, c], 0.0)
        mixed = taps[2][:, c] * window[8:, c] + taps[1][:, c] * back1 + taps[0][:, c] * back2
        parts.append((g_out[:, c].astype(F32) * mixed).astype(BF16))
    return parts


def slots_kernel(iv, onehot, pick):
    tokens = iv.shape[1]
    first = iv[0:1, :]
    second = iv[1:2, :]
    expert = lax.broadcasted_iota(jnp.int32, (128, tokens), 0)
    m0 = (expert == first).astype(F32)
    m1 = (expert == second).astype(F32)
    r = lax.broadcasted_iota(jnp.int32, (tokens, tokens), 0)
    c = lax.broadcasted_iota(jnp.int32, (tokens, tokens), 1)
    before = (r < c).astype(F32).astype(BF16)
    n0 = dot(m0.astype(BF16), before)
    n1 = dot(m1.astype(BF16), before) + jnp.sum(m0, axis=1, keepdims=True)
    rank0 = jnp.sum(m0 * n0, axis=0, keepdims=True).astype(jnp.int32)
    rank1 = jnp.sum(m1 * n1, axis=0, keepdims=True).astype(jnp.int32)
    target = [first * 8 + rank0, second * 8 + rank1]
    slots = onehot.shape[0]
    row = lax.broadcasted_iota(jnp.int32, (slots, tokens), 0)
    onehot[:, 0:tokens] = ((row == target[0]) | (row == target[1])).astype(F32).astype(BF16)
    onehot[:, tokens:] = ((row == target[0] + 4) | (row == target[1] + 4)).astype(F32).astype(BF16)
    for k, (chosen, rank) in enumerate(((first, rank0), (second, rank1))):
        line = jnp.broadcast_to((chosen * 4 + rank).astype(F32), (128, tokens)).T
        for n in range(pick.shape[1] // 128):
            lane = (lax.broadcasted_iota(jnp.int32, (tokens, 128), 1) + 128 * n).astype(F32)
            span = slice(128 * n, 128 * n + 128)
            pick[k * tokens : (k + 1) * tokens, span] = (line == lane).astype(F32).astype(BF16)


def early_kernel(place, xv, gv, ov, taps, dv, o0, o1, o2, o3, head, head_ids, gate_v, taps_v, prod, doc_col):
    rows = xv.shape[0]
    part = o0.shape[0]
    taps_v[...] = taps[...]
    prod[0:8, :] = jnp.zeros((8, xv.shape[1]), F32)
    prod[8:, :] = xv[...].astype(F32) * gv[...].astype(F32)
    doc_col[0:8, :] = jnp.zeros((8, 128), F32)
    for block in range(rows // 128):
        line = jnp.broadcast_to(dv[block : block + 1, :].astype(F32), (128, 128))
        doc_col[8 + 128 * block : 136 + 128 * block, :] = line.T
    head[...] = prod[8:24, :]
    head_ids[...] = doc_col[8:24, :]
    gate_v[...] = ov[0:16, :]
    weights = taps_of(taps_v)
    here = place[0]
    for shift, out in enumerate((o0, o1, o2, o3)):
        start = pl.multiple_of(lax.rem(here + shift, 4) * part, part)
        pieces = conv_rows(
            prod[pl.ds(start, part + 8), :], doc_col[pl.ds(start, part + 8), :],
            ov[pl.ds(start, part), :], weights,
        )
        for half, piece in enumerate(pieces):
            out[:, 128 * half : 128 * half + 128] = piece


def fix_kernel(place, earlier, head, head_ids, g_out, taps, i0, i1, i2, i3, o0, o1, o2, o3):
    width = head.shape[1]
    part = i0.shape[0]
    here = place[0]
    window = jnp.concatenate([jnp.zeros((6, width), F32), earlier[0:2, :], head[...]], axis=0)
    before = [jnp.broadcast_to(earlier[2:3, k : k + 1], (1, 128)) for k in (126, 127)]
    ids = jnp.concatenate([jnp.zeros((6, 128), F32), *before, head_ids[...]], axis=0)
    pieces = conv_rows(window, ids, g_out[...], taps_of(taps))
    for shift, (old, out) in enumerate(zip((i0, i1, i2, i3), (o0, o1, o2, o3))):
        out[16:part, :] = old[16:part, :]
        mine = jnp.full((16, 128), lax.rem(here + shift, 4), jnp.int32) == 0
        for half, piece in enumerate(pieces):
            c = slice(128 * half, 128 * half + 128)
            out[0:16, c] = jnp.where(mine, piece.astype(F32), old[0:16, c].astype(F32)).astype(BF16)


def mix_kernel(place, r0, r1, r2, r3, residual, proj, gain, onehot, buf, carried, halves, joined):
    here = place[0]
    width = residual.shape[1]
    half = width // 2
    tokens = residual.shape[0]
    for shift, part in enumerate((r0, r1, r2, r3)):
        depth = part.shape[1]
        start = pl.multiple_of(lax.rem(here + 4 - shift, 4) * depth, depth)
        joined[:, pl.ds(start, depth)] = part[...]
    step = 512
    total = jnp.zeros((tokens, 1), F32)
    for n in range(width // step):
        c = slice(n * step, n * step + step)
        acc = dot(joined[...], proj[:, c])
        value = residual[:, c].astype(F32) + acc.astype(BF16).astype(F32)
        carried[:, c] = value
        total = total + jnp.sum(value * value, axis=1, keepdims=True)
    scale = lax.rsqrt(total * (1.0 / width) + 1e-06)
    for n in range(width // step):
        c = slice(n * step, n * step + step)
        value = (carried[:, c] * scale * gain[:, c]).astype(BF16)
        h = (n * step) // half
        halves[h * tokens : (h + 1) * tokens, n * step - h * half : n * step - h * half + step] = value
    for n in range(half // 256):
        c = slice(n * 256, n * 256 + 256)
        buf[:, c] = dot(onehot[...], halves[:, c]).astype(BF16)


def expert_kernel(arrived, wg, wu, wd, out, xv, hv):
    rows, half = arrived.shape
    blocks = wg.shape[1] // 256
    cols = [slice(256 * j, 256 * j + 256) for j in range(blocks)]
    low = lax.broadcasted_iota(jnp.int32, (rows // 16, 8, 256), 1) < 4
    for j, c in enumerate(cols):
        value = arrived[:, c].astype(F32).reshape(rows // 16, 2, 8, 256)
        even, odd = value[:, 0], value[:, 1]
        lo = jnp.where(low, even, pltpu.roll(odd, 4, 1))
        hi = jnp.where(low, pltpu.roll(even, 4, 1), odd)
        xv[:, c] = lo.reshape(rows // 2, 256).astype(BF16)
        xv[:, half + 256 * j : half + 256 * j + 256] = hi.reshape(rows // 2, 256).astype(BF16)
    for j, c in enumerate(cols):
        gate = dot(xv[...], wg[:, c])
        up = dot(xv[...], wu[:, c])
        hv[:, c] = (gate / (1.0 + jnp.exp(-gate)) * up).astype(BF16)
    for j, c in enumerate(cols):
        lo = dot(hv[...], wd[:, c]).reshape(rows // 16, 8, 256)
        hi = dot(hv[...], wd[:, half + 256 * j : half + 256 * j + 256]).reshape(rows // 16, 8, 256)
        even = jnp.where(low, lo, pltpu.roll(hi, 4, 1))
        odd = jnp.where(low, pltpu.roll(lo, 4, 1), hi)
        out[:, c] = jnp.stack([even, odd], axis=1).reshape(rows, 256).astype(BF16)


def combine_kernel(returned, carried, pick, weights, out, ov, sem):
    tokens = carried.shape[0]
    rows, half = returned.shape
    w = [jnp.broadcast_to(weights[k : k + 1, :], (128, tokens)).T[:, 0:1] for k in range(2)]
    low = lax.broadcasted_iota(jnp.int32, (rows // 16, 8, 256), 1) < 4
    copies = []
    for n in range(half // 256):
        c = slice(256 * n, 256 * n + 256)
        value = returned[:, c].astype(F32).reshape(rows // 16, 2, 8, 256)
        even, odd = value[:, 0], value[:, 1]
        lo = jnp.where(low, even, pltpu.roll(odd, 4, 1))
        hi = jnp.where(low, pltpu.roll(even, 4, 1), odd)
        for h, source in enumerate((lo, hi)):
            d = slice(h * half + 256 * n, h * half + 256 * n + 256)
            both = dot(pick[...], source.reshape(rows // 2, 256).astype(BF16))
            ov[:, d] = (carried[:, d] + (w[0] * both[:tokens] + w[1] * both[tokens:])).astype(BF16)
            copy = pltpu.make_async_copy(ov.at[:, d], out.at[:, d], sem.at[len(copies)])
            copy.start()
            copies.append(copy)
    for copy in copies:
        copy.wait()


def call(kernel, out_shape, in_specs, out_specs, scratch, vmem_mib, flops=0, nbytes=0, name=None):
    return pl.pallas_call(
        kernel,
        out_shape=out_shape,
        in_specs=in_specs,
        out_specs=out_specs,
        scratch_shapes=scratch,
        name=name,
        compiler_params=pltpu.CompilerParams(vmem_limit_bytes=int(vmem_mib * 1048576)),
        cost_estimate=pl.CostEstimate(flops=flops, bytes_accessed=nbytes, transcendentals=0),
    )


def shape(dims, kind):
    return jax.ShapeDtypeStruct(dims, kind)


def on_device(conv_input, gate_inner, gate_outer, conv_taps, doc_ids, residual_in, out_proj,
              norm_gain, expert_ids, expert_weights, gate_proj, up_proj, down_proj):
    length, channels = conv_input.shape
    tokens, width = residual_in.shape
    sp_count = lax.axis_size("sp")
    tp_count = lax.axis_size("tp")
    experts = sp_count * tp_count
    place = lax.axis_index("tp").reshape(1)
    docs = doc_ids.reshape(-1, 128)
    edge = call(
        edge_kernel, pltpu.VMEM((4, channels), F32), [HB] * 3, VM,
        [pltpu.VMEM((16, channels), BF16), pltpu.VMEM((16, channels), BF16),
         pltpu.VMEM(docs.shape, jnp.int32), pltpu.SemaphoreType.DMA((3,))],
        EDGE, EDGE_FLOPS, 1 << 16, name="edge",
    )(conv_input, gate_inner, docs)
    earlier = lax.ppermute(edge, "sp", [(i, i + 1) for i in range(sp_count - 1)])
    gain = norm_gain.reshape(1, -1)
    rows = experts * 8
    half = width // 2
    piece = pltpu.VMEM((tokens, channels), BF16)
    outs = (piece,) * 4 + (
        pltpu.VMEM((16, channels), F32), pltpu.VMEM((16, 128), F32), pltpu.VMEM((16, channels), BF16),
        pltpu.VMEM(conv_taps.shape, BF16),
    )
    *raw, head, head_ids, gate_v, taps_v = call(
        early_kernel, outs, [SM] + [VM] * 5, (VM,) * len(outs),
        [pltpu.VMEM((length + 8, channels), F32), pltpu.VMEM((length + 8, 128), F32)],
        EARLY, EARLY_FLOPS, 1 << 20, name="early",
    )(place, conv_input, gate_inner, gate_outer, conv_taps, docs)
    sent = call(
        fix_kernel, (piece,) * 4, [SM] + [VM] * 9, (VM,) * 4, [], 4, 1 << 20, 1 << 18,
        name="fix",
    )(place, earlier, head, head_ids, gate_v, taps_v, *raw)
    parts = [sent[0], None, None, None]
    for d in ORDER:
        parts[d] = lax.ppermute(sent[d], "tp", [(i, (i + d) % tp_count) for i in range(tp_count)])
    held = (pltpu.VMEM((rows, 2 * tokens), BF16), pltpu.VMEM((2 * tokens, rows // 2), BF16))
    onehot, pick = call(
        slots_kernel, held, [VM], (VM,) * 2, [], SLOTS, SLOT_FLOPS, 1 << 20, name="slots",
    )(expert_ids.T)
    buf, carried = call(
        mix_kernel, (shape((rows, half), BF16), shape((tokens, width), F32)),
        [SM] + [VM] * 8, (VM, VM),
        [pltpu.VMEM((2 * tokens, half), BF16), pltpu.VMEM((tokens, out_proj.shape[0]), BF16)],
        12, 8 << 30, 1 << 23, name="mix",
    )(place, *parts, residual_in, out_proj, gain, onehot)
    arrived = lax.all_to_all(buf.reshape(experts, 8, half), ("sp", "tp"), split_axis=0, concat_axis=0, tiled=True)
    hidden = gate_proj.shape[2]
    result = call(
        expert_kernel, shape((rows, half), BF16), [VM] * 4, VM,
        [
            pltpu.VMEM((rows // 2, width), BF16),
            pltpu.VMEM((rows // 2, hidden), BF16),
        ],
        20, 6 << 30, 1 << 24, name="experts",
    )(arrived.reshape(rows, half), gate_proj[0], up_proj[0], down_proj[0])
    returned = lax.all_to_all(result.reshape(experts, 8, half), ("sp", "tp"), split_axis=0, concat_axis=0, tiled=True)
    return call(
        combine_kernel, shape((tokens, width), BF16), [VM] * 4, HB,
        [pltpu.VMEM((tokens, width), BF16), pltpu.SemaphoreType.DMA((8,))],
        12, 1 << 30, 1 << 22, name="combine",
    )(returned.reshape(rows, half), carried, pick, expert_weights.T)


def solution(mesh):
    both = ("sp", "tp")
    in_specs = (
        P("sp", "tp"),
        P("sp", "tp"),
        P("sp", "tp"),
        P(None, "tp"),
        P("sp"),
        P(both, None),
        P(),
        P(),
        P(both, None),
        P(both, None),
        P(both, None, None),
        P(both, None, None),
        P(both, None, None),
    )
    return jax.shard_map(
        on_device, mesh=mesh, in_specs=in_specs, out_specs=P(both, None), check_vma=False
    )
```

```python
import functools
import jax
import jax.numpy as jnp
from jax import lax
from jax.experimental import pallas as pl
from jax.experimental.pallas import tpu as pltpu
from jax.sharding import PartitionSpec as P

F32 = jnp.float32
BF16 = jnp.bfloat16
EDGE = 61
EARLY = 24
SLOTS = 8
SLOT_FLOPS = 2 << 30
EARLY_FLOPS = 8 << 30
EDGE_FLOPS = 8 << 30
ORDER = (1, 2, 3)
VM = pl.BlockSpec(memory_space=pltpu.VMEM)
SM = pl.BlockSpec(memory_space=pltpu.SMEM)
HB = pl.BlockSpec(memory_space=pl.ANY)


def dot(a, b):
    return jnp.dot(a, b, preferred_element_type=F32)


def edge_kernel(x, g_in, docs, out, xv, gv, dv, sem):
    rows = x.shape[0]
    copies = [
        pltpu.make_async_copy(x.at[rows - 16 :, :], xv, sem.at[0]),
        pltpu.make_async_copy(g_in.at[rows - 16 :, :], gv, sem.at[1]),
        pltpu.make_async_copy(docs, dv, sem.at[2]),
    ]
    for copy in copies:
        copy.start()
    for copy in copies:
        copy.wait()
    prod = xv[...].astype(F32) * gv[...].astype(F32)
    last = dv.shape[0] - 1
    out[0:2, :] = prod[14:16, :]
    for c in range(out.shape[1] // 128):
        out[2:4, 128 * c : 128 * c + 128] = jnp.broadcast_to(dv[last : last + 1, :].astype(F32), (2, 128))


def taps_of(taps):
    return [taps[k : k + 1, :].astype(F32) for k in range(3)]


def conv_rows(window, ids, g_out, taps):
    count = window.shape[0] - 8
    cur = ids[8:]
    parts = []
    for half in range(window.shape[1] // 128):
        c = slice(128 * half, 128 * half + 128)
        back1 = jnp.where(ids[7:-1] == cur, window[7:-1, c], 0.0)
        back2 = jnp.where(ids[6:-2] == cur, window[6:-2, c], 0.0)
        mixed = taps[2][:, c] * window[8:, c] + taps[1][:, c] * back1 + taps[0][:, c] * back2
        parts.append((g_out[:, c].astype(F32) * mixed).astype(BF16))
    return parts


def slots_kernel(iv, onehot, pick):
    tokens = iv.shape[1]
    first = iv[0:1, :]
    second = iv[1:2, :]
    expert = lax.broadcasted_iota(jnp.int32, (128, tokens), 0)
    m0 = (expert == first).astype(F32)
    m1 = (expert == second).astype(F32)
    r = lax.broadcasted_iota(jnp.int32, (tokens, tokens), 0)
    c = lax.broadcasted_iota(jnp.int32, (tokens, tokens), 1)
    before = (r < c).astype(F32).astype(BF16)
    n0 = dot(m0.astype(BF16), before)
    n1 = dot(m1.astype(BF16), before) + jnp.sum(m0, axis=1, keepdims=True)
    rank0 = jnp.sum(m0 * n0, axis=0, keepdims=True).astype(jnp.int32)
    rank1 = jnp.sum(m1 * n1, axis=0, keepdims=True).astype(jnp.int32)
    target = [first * 8 + rank0, second * 8 + rank1]
    slots = onehot.shape[0]
    row = lax.broadcasted_iota(jnp.int32, (slots, tokens), 0)
    onehot[:, 0:tokens] = ((row == target[0]) | (row == target[1])).astype(F32).astype(BF16)
    onehot[:, tokens:] = ((row == target[0] + 4) | (row == target[1] + 4)).astype(F32).astype(BF16)
    for k, (chosen, rank) in enumerate(((first, rank0), (second, rank1))):
        line = jnp.broadcast_to((chosen * 4 + rank).astype(F32), (128, tokens)).T
        for n in range(pick.shape[1] // 128):
            lane = (lax.broadcasted_iota(jnp.int32, (tokens, 128), 1) + 128 * n).astype(F32)
            span = slice(128 * n, 128 * n + 128)
            pick[k * tokens : (k + 1) * tokens, span] = (line == lane).astype(F32).astype(BF16)


def early_kernel(place, xv, gv, ov, taps, dv, o0, o1, o2, o3, head, head_ids, gate_v, taps_v, prod, doc_col):
    rows = xv.shape[0]
    part = o0.shape[0]
    taps_v[...] = taps[...]
    prod[0:8, :] = jnp.zeros((8, xv.shape[1]), F32)
    prod[8:, :] = xv[...].astype(F32) * gv[...].astype(F32)
    doc_col[0:8, :] = jnp.zeros((8, 128), F32)
    for block in range(rows // 128):
        line = jnp.broadcast_to(dv[block : block + 1, :].astype(F32), (128, 128))
        doc_col[8 + 128 * block : 136 + 128 * block, :] = line.T
    head[...] = prod[8:24, :]
    head_ids[...] = doc_col[8:24, :]
    gate_v[...] = ov[0:16, :]
    weights = taps_of(taps_v)
    here = place[0]
    for shift, out in enumerate((o0, o1, o2, o3)):
        start = pl.multiple_of(lax.rem(here + shift, 4) * part, part)
        pieces = conv_rows(
            prod[pl.ds(start, part + 8), :], doc_col[pl.ds(start, part + 8), :],
            ov[pl.ds(start, part), :], weights,
        )
        for half, piece in enumerate(pieces):
            out[:, 128 * half : 128 * half + 128] = piece


def fix_kernel(place, earlier, head, head_ids, g_out, taps, i0, i1, i2, i3, o0, o1, o2, o3):
    width = head.shape[1]
    part = i0.shape[0]
    here = place[0]
    window = jnp.concatenate([jnp.zeros((6, width), F32), earlier[0:2, :], head[...]], axis=0)
    before = [jnp.broadcast_to(earlier[2:3, k : k + 1], (1, 128)) for k in (126, 127)]
    ids = jnp.concatenate([jnp.zeros((6, 128), F32), *before, head_ids[...]], axis=0)
    pieces = conv_rows(window, ids, g_out[...], taps_of(taps))
    for shift, (old, out) in enumerate(zip((i0, i1, i2, i3), (o0, o1, o2, o3))):
        out[16:part, :] = old[16:part, :]
        mine = jnp.full((16, 128), lax.rem(here + shift, 4), jnp.int32) == 0
        for half, piece in enumerate(pieces):
            c = slice(128 * half, 128 * half + 128)
            out[0:16, c] = jnp.where(mine, piece.astype(F32), old[0:16, c].astype(F32)).astype(BF16)


def mix_kernel(place, r0, r1, r2, r3, residual, proj, gain, onehot, buf, carried, halves, joined):
    here = place[0]
    width = residual.shape[1]
    half = width // 2
    tokens = residual.shape[0]
    for shift, part in enumerate((r0, r1, r2, r3)):
        depth = part.shape[1]
        start = pl.multiple_of(lax.rem(here + 4 - shift, 4) * depth, depth)
        joined[:, pl.ds(start, depth)] = part[...]
    step = 512
    total = jnp.zeros((tokens, 1), F32)
    for n in range(width // step):
        c = slice(n * step, n * step + step)
        acc = dot(joined[...], proj[:, c])
        value = residual[:, c].astype(F32) + acc.astype(BF16).astype(F32)
        carried[:, c] = value
        total = total + jnp.sum(value * value, axis=1, keepdims=True)
    scale = lax.rsqrt(total * (1.0 / width) + 1e-06)
    for n in range(width // step):
        c = slice(n * step, n * step + step)
        value = (carried[:, c] * scale * gain[:, c]).astype(BF16)
        h = (n * step) // half
        halves[h * tokens : (h + 1) * tokens, n * step - h * half : n * step - h * half + step] = value
    for n in range(half // 256):
        c = slice(n * 256, n * 256 + 256)
        buf[:, c] = dot(onehot[...], halves[:, c]).astype(BF16)


def expert_kernel(arrived, wg, wu, wd, out, xv, hv):
    rows, half = arrived.shape
    blocks = wg.shape[1] // 256
    cols = [slice(256 * j, 256 * j + 256) for j in range(blocks)]
    low = lax.broadcasted_iota(jnp.int32, (rows // 16, 8, 256), 1) < 4
    for j, c in enumerate(cols):
        value = arrived[:, c].astype(F32).reshape(rows // 16, 2, 8, 256)
        even, odd = value[:, 0], value[:, 1]
        lo = jnp.where(low, even, pltpu.roll(odd, 4, 1))
        hi = jnp.where(low, pltpu.roll(even, 4, 1), odd)
        xv[:, c] = lo.reshape(rows // 2, 256).astype(BF16)
        xv[:, half + 256 * j : half + 256 * j + 256] = hi.reshape(rows // 2, 256).astype(BF16)
    for j, c in enumerate(cols):
        gate = dot(xv[...], wg[:, c])
        up = dot(xv[...], wu[:, c])
        hv[:, c] = (gate / (1.0 + jnp.exp(-gate)) * up).astype(BF16)
    for j, c in enumerate(cols):
        lo = dot(hv[...], wd[:, c]).reshape(rows // 16, 8, 256)
        hi = dot(hv[...], wd[:, half + 256 * j : half + 256 * j + 256]).reshape(rows // 16, 8, 256)
        even = jnp.where(low, lo, pltpu.roll(hi, 4, 1))
        odd = jnp.where(low, pltpu.roll(lo, 4, 1), hi)
        out[:, c] = jnp.stack([even, odd], axis=1).reshape(rows, 256).astype(BF16)


def combine_kernel(returned, carried, pick, weights, out, ov, sem):
    tokens = carried.shape[0]
    rows, half = returned.shape
    w = [jnp.broadcast_to(weights[k : k + 1, :], (128, tokens)).T[:, 0:1] for k in range(2)]
    low = lax.broadcasted_iota(jnp.int32, (rows // 16, 8, 256), 1) < 4
    copies = []
    for n in range(half // 256):
        c = slice(256 * n, 256 * n + 256)
        value = returned[:, c].astype(F32).reshape(rows // 16, 2, 8, 256)
        even, odd = value[:, 0], value[:, 1]
        lo = jnp.where(low, even, pltpu.roll(odd, 4, 1))
        hi = jnp.where(low, pltpu.roll(even, 4, 1), odd)
        for h, source in enumerate((lo, hi)):
            d = slice(h * half + 256 * n, h * half + 256 * n + 256)
            both = dot(pick[...], source.reshape(rows // 2, 256).astype(BF16))
            ov[:, d] = (carried[:, d] + (w[0] * both[:tokens] + w[1] * both[tokens:])).astype(BF16)
            copy = pltpu.make_async_copy(ov.at[:, d], out.at[:, d], sem.at[len(copies)])
            copy.start()
            copies.append(copy)
    for copy in copies:
        copy.wait()


def call(kernel, out_shape, in_specs, out_specs, scratch, vmem_mib, flops=0, nbytes=0, name=None):
    return pl.pallas_call(
        kernel,
        out_shape=out_shape,
        in_specs=in_specs,
        out_specs=out_specs,
        scratch_shapes=scratch,
        name=name,
        compiler_params=pltpu.CompilerParams(vmem_limit_bytes=int(vmem_mib * 1048576)),
        cost_estimate=pl.CostEstimate(flops=flops, bytes_accessed=nbytes, transcendentals=0),
    )


def shape(dims, kind):
    return jax.ShapeDtypeStruct(dims, kind)


def on_device(conv_input, gate_inner, gate_outer, conv_taps, doc_ids, residual_in, out_proj,
              norm_gain, expert_ids, expert_weights, gate_proj, up_proj, down_proj):
    length, channels = conv_input.shape
    tokens, width = residual_in.shape
    sp_count = lax.axis_size("sp")
    tp_count = lax.axis_size("tp")
    experts = sp_count * tp_count
    place = lax.axis_index("tp").reshape(1)
    docs = doc_ids.reshape(-1, 128)
    edge = call(
        edge_kernel, pltpu.VMEM((4, channels), F32), [HB] * 3, VM,
        [pltpu.VMEM((16, channels), BF16), pltpu.VMEM((16, channels), BF16),
         pltpu.VMEM(docs.shape, jnp.int32), pltpu.SemaphoreType.DMA((3,))],
        EDGE, EDGE_FLOPS, 1 << 16, name="edge",
    )(conv_input, gate_inner, docs)
    earlier = lax.ppermute(edge, "sp", [(i, i + 1) for i in range(sp_count - 1)])
    gain = norm_gain.reshape(1, -1)
    rows = experts * 8
    half = width // 2
    piece = pltpu.VMEM((tokens, channels), BF16)
    outs = (piece,) * 4 + (
        pltpu.VMEM((16, channels), F32), pltpu.VMEM((16, 128), F32), pltpu.VMEM((16, channels), BF16),
        pltpu.VMEM(conv_taps.shape, BF16),
    )
    *raw, head, head_ids, gate_v, taps_v = call(
        early_kernel, outs, [SM] + [VM] * 5, (VM,) * len(outs),
        [pltpu.VMEM((length + 8, channels), F32), pltpu.VMEM((length + 8, 128), F32)],
        EARLY, EARLY_FLOPS, 1 << 20, name="early",
    )(place, conv_input, gate_inner, gate_outer, conv_taps, docs)
    sent = call(
        fix_kernel, (piece,) * 4, [SM] + [VM] * 9, (VM,) * 4, [], 4, 1 << 20, 1 << 18,
        name="fix",
    )(place, earlier, head, head_ids, gate_v, taps_v, *raw)
    parts = [sent[0], None, None, None]
    for d in ORDER:
        parts[d] = lax.ppermute(sent[d], "tp", [(i, (i + d) % tp_count) for i in range(tp_count)])
    held = (pltpu.VMEM((rows, 2 * tokens), BF16), pltpu.VMEM((2 * tokens, rows // 2), BF16))
    onehot, pick = call(
        slots_kernel, held, [VM], (VM,) * 2, [], SLOTS, SLOT_FLOPS, 1 << 20, name="slots",
    )(expert_ids.T)
    buf, carried = call(
        mix_kernel, (shape((rows, half), BF16), shape((tokens, width), F32)),
        [SM] + [VM] * 8, (VM, VM),
        [pltpu.VMEM((2 * tokens, half), BF16), pltpu.VMEM((tokens, out_proj.shape[0]), BF16)],
        12, 8 << 30, 1 << 23, name="mix",
    )(place, *parts, residual_in, out_proj, gain, onehot)
    arrived = lax.all_to_all(buf.reshape(experts, 8, half), ("sp", "tp"), split_axis=0, concat_axis=0, tiled=True)
    hidden = gate_proj.shape[2]
    result = call(
        expert_kernel, shape((rows, half), BF16), [VM] * 4, VM,
        [
            pltpu.VMEM((rows // 2, width), BF16),
            pltpu.VMEM((rows // 2, hidden), BF16),
        ],
        20, 6 << 30, 1 << 24, name="experts",
    )(arrived.reshape(rows, half), gate_proj[0], up_proj[0], down_proj[0])
    returned = lax.all_to_all(result.reshape(experts, 8, half), ("sp", "tp"), split_axis=0, concat_axis=0, tiled=True)
    return call(
        combine_kernel, shape((tokens, width), BF16), [VM] * 4, HB,
        [pltpu.VMEM((tokens, width), BF16), pltpu.SemaphoreType.DMA((8,))],
        12, 1 << 30, 1 << 22, name="combine",
    )(returned.reshape(rows, half), carried, pick, expert_weights.T)


def solution(mesh):
    both = ("sp", "tp")
    in_specs = (
        P("sp", "tp"),
        P("sp", "tp"),
        P("sp", "tp"),
        P(None, "tp"),
        P("sp"),
        P(both, None),
        P(),
        P(),
        P(both, None),
        P(both, None),
        P(both, None, None),
        P(both, None, None),
        P(both, None, None),
    )
    return jax.shard_map(
        on_device, mesh=mesh, in_specs=in_specs, out_specs=P(both, None), check_vma=False
    )
```
